32 devices in a mesh: ep: 16 (over z, y, x), tp: 2 (over core).
Axes of the slice: x: 2, y: 2, z: 4, core: 2. Of those that a mesh axis runs over, the one named last changes fastest.
Arguments:
- tokens: bfloat16 [256, 2048], P('ep'), may hold values from -6 to 6
- mix_gain: float32 [2048], replicated, may hold values from 0.1 to 1.9
- query_weight: bfloat16 [2048, 1024], P('ep', 'tp'), may hold values from -0.125 to 0.125
- forget_weight: bfloat16 [2048, 1024], P('ep', 'tp'), may hold values from -0.125 to 0.125
- input_weight: bfloat16 [2048, 1024], P('ep', 'tp'), may hold values from -0.125 to 0.125
- lower_bound: float32 [1024], P('tp'), may hold values from 0 to 0.9
- head_gain: float32 [1024], P('tp'), may hold values from 0.1 to 1.9
- out_weight: bfloat16 [1024, 2048], P('tp', 'ep'), may hold values from -0.1875 to 0.1875
- state: float32 [256, 8, 128, 128], P('ep', 'tp'), may hold values from -4 to 4
- ffn_gain: float32 [2048], replicated, may hold values from 0.1 to 1.9
- route_ids: int32 [256, 2], P('ep'), may hold values from 0 to 7, all different within a row; in each aligned block of 16 rows (0 to 15, 16 to 31, ...) at most 6 rows name the same one
- route_weights: float32 [256, 2], P('ep'), may hold values from 0.25 to 1
- expert_gate: bfloat16 [16, 2048, 2048], P('ep', None, 'tp'), may hold values from -0.125 to 0.125
- expert_up: bfloat16 [16, 2048, 2048], P('ep', None, 'tp'), may hold values from -0.125 to 0.125
- expert_down: bfloat16 [16, 2048, 2048], P('ep', 'tp'), may hold values from -0.09375 to 0.09375
Outputs:
- mixed_out: bfloat16 [256, 2048], P('ep', 'tp')
- new_state: float32 [256, 8, 128, 128], P('ep', 'tp')
The draws below stay inside these ranges and needn't reach their ends.
Inputs may be any that keep to these rules, and one draw needn't show every extreme that they name: `route_ids`: each row names 2 different experts; among the rows of one device no expert is named by more than 6 rows, a bound that some block reaches of them.
All inputs are finite; a program needn't handle non-finite values.
Results may differ from the reference program's by a relative error of at most 0.015.
Values may be sent and summed in bfloat16 or wider, within the bound.
No kernel may reach another device: no remote copies, remote signals or barrier semaphores. Data moves between devices by JAX's collectives and lax.ppermute only.
A program may use at most 64 MiB of HBM per device.

```python
import math
import jax
import jax.numpy as jnp
import numpy as np
from jax import lax

D = 2048
HEADS = 8
HEAD_DIM = 128
FF_E = 4096
EXPERTS = 8
TOP = 2
SEQ_DEV = 16
CAP = 6
SEQS = 256
SPAN = 2
N_EP = 16
N_TP = 2


def steps_of(own_key, extent, shards, smallest, high):
    def one(position, shards_of):
        steps = jax.random.uniform(jax.random.fold_in(jax.random.fold_in(own_key, 6), position), (shards_of,), jnp.float32, smallest / len(shards), high / len(shards))
        return jnp.repeat(jnp.exp(steps), extent[position] // shards_of).reshape((-1,) + (1,) * (len(extent) - position - 1))

    level = one(*shards[0])
    for cut in shards[1:]:
        level = level * one(*cut)
    return level


def assign_block(own_key, own, number, rows, count, top, bound, slope):
    ranking = jax.random.permutation(own_key, count)
    packed, ordinary = portions_of(count, rows * top, bound, slope, True), portions_of(count, rows * top, bound, slope, False)
    places = jnp.arange(count)

    def named(tallies, rotation):
        used = int((tallies > 0).sum())
        fixed = max(1, used // 4)
        moved = fixed + (places - fixed + rotation * (used - fixed)) % max(1, count - fixed)
        return jnp.zeros((count,), jnp.int32).at[ranking[jnp.where(places < fixed, places, moved)]].set(jnp.asarray(tallies, jnp.int32))

    tallies = jnp.where(number % 4 == 0, named(packed, number // 4), named(ordinary, number - number // 4 - 1))
    mixed = jax.random.permutation(jax.random.fold_in(own, 3), count)
    giver, receiver = mixed[0:count // 2 * 2:2], mixed[1:count // 2 * 2:2]
    margin = jnp.minimum(tallies[giver] - 1, bound - tallies[receiver]) // 2
    margin = jnp.where((giver == ranking[0]) | (receiver == ranking[0]) | (tallies[receiver] == 0), 0, jnp.maximum(margin, 0))
    moved = jax.random.randint(jax.random.fold_in(own, 4), (count // 2,), 0, 1 << 20) % (margin + 1)
    tallies = tallies.at[giver].add(-moved).at[receiver].add(moved)
    labels = jnp.searchsorted(jnp.cumsum(tallies), jnp.arange(rows * top), side="right").astype(jnp.int32)
    grid = labels.reshape(top, rows).T
    grid = grid[jax.random.permutation(jax.random.fold_in(own, 1), rows)]
    rotation = jax.random.randint(jax.random.fold_in(own, 2), (rows, 1), 0, top)
    return jnp.take_along_axis(grid, (jnp.arange(top)[None, :] + rotation) % top, axis=1)


def portions_of(count, total, reach, slope, full):
    weights = [(1 << 20) // math.isqrt(rank ** slope) + 1 for rank in range(1, count + 1)]
    largest = reach if full else min(reach, max(-(-total // count), total * weights[0] // sum(weights)))
    least = 1 if total - largest >= count - 1 else 0
    counts, rest = [largest] + [least] * (count - 1), total - largest - least * (count - 1)
    while rest > 0:
        movable = [i for i in range(1, count) if counts[i] < largest] or [i for i in range(1, count) if counts[i] < reach]
        mass, budget = sum([weights[i] for i in movable]), rest
        for i in movable:
            extra = min(reach - counts[i], max(1, budget * weights[i] // mass), rest)
            counts[i] = counts[i] + extra
            rest = rest - extra
    return np.array(counts)


def centred(own_key, extent, spread, limit, shards=(), held_as=jnp.bfloat16):
    values = spread * jax.random.normal(own_key, extent, jnp.float32)
    if shards:
        values = values * steps_of(own_key, extent, shards, -0.22, 0.18)
    return jnp.clip(values, -limit, limit).astype(held_as)


def setup_inputs(seed: int = 0) -> dict:
    arg_keys = jax.random.split(jax.random.key(seed), 16)
    tokens = centred(arg_keys[0], (SEQS, D), 1.0, 6.0, ((0, 16),))
    mix_gain = jnp.clip(1.0 + 0.18 * jax.random.normal(arg_keys[1], (D,), jnp.float32), 0.1, 1.9)
    query_weight = centred(arg_keys[2], (D, HEADS * HEAD_DIM), D ** -0.5, 0.125, ((0, 16), (1, 2)))
    forget_weight = centred(arg_keys[3], (D, HEADS * HEAD_DIM), D ** -0.5, 0.125, ((0, 16), (1, 2)))
    input_weight = centred(arg_keys[4], (D, HEADS * HEAD_DIM), D ** -0.5, 0.125, ((0, 16), (1, 2)))
    lower_bound = jnp.clip(0.9 * jax.random.uniform(arg_keys[5], (HEADS * HEAD_DIM,), jnp.float32) ** steps_of(arg_keys[5], (HEADS * HEAD_DIM,), ((0, 2),), -0.2, 0.2), 0.0, 0.9)
    head_gain = jnp.clip(1.0 + 0.18 * jax.random.normal(arg_keys[6], (HEADS * HEAD_DIM,), jnp.float32), 0.1, 1.9)
    out_weight = centred(arg_keys[7], (HEADS * HEAD_DIM, D), (HEADS * HEAD_DIM) ** -0.5, 0.1875, ((0, 2), (1, 16)))
    state = centred(arg_keys[8], (SEQS, HEADS, HEAD_DIM, HEAD_DIM), 0.5, 4.0, ((0, 16), (1, 2)), jnp.float32)
    ffn_gain = jnp.clip(1.0 + 0.18 * jax.random.normal(arg_keys[9], (D,), jnp.float32), 0.1, 1.9)
    route_ids_keys = jax.random.split(jax.random.fold_in(arg_keys[10], 1), SEQS // SEQ_DEV)
    route_ids_turns = jax.random.permutation(jax.random.fold_in(arg_keys[10], 3), SEQS // SEQ_DEV)
    route_ids = jax.vmap(lambda own, number: assign_block(jax.random.fold_in(arg_keys[10], 2), own, number, SEQ_DEV, EXPERTS, TOP, CAP, 2))(route_ids_keys, route_ids_turns).reshape((SEQS, TOP))
    route_weights = jnp.clip(0.25 + 0.75 * jax.random.uniform(arg_keys[11], (SEQS, TOP), jnp.float32) ** steps_of(arg_keys[11], (SEQS, TOP), ((0, 16),), -0.2, 0.2), 0.25, 1.0)
    expert_gate = centred(arg_keys[12], (EXPERTS * SPAN, D, FF_E // SPAN), D ** -0.5, 0.125, ((0, 16), (2, 2)))
    expert_up = centred(arg_keys[13], (EXPERTS * SPAN, D, FF_E // SPAN), D ** -0.5, 0.125, ((0, 16), (2, 2)))
    expert_down = centred(arg_keys[14], (EXPERTS * SPAN, FF_E // SPAN, D), FF_E ** -0.5, 0.09375, ((0, 16), (1, 2)))
    return {"tokens": tokens, "mix_gain": mix_gain, "query_weight": query_weight, "forget_weight": forget_weight, "input_weight": input_weight, "lower_bound": lower_bound, "head_gain": head_gain, "out_weight": out_weight, "state": state, "ffn_gain": ffn_gain, "route_ids": route_ids, "route_weights": route_weights, "expert_gate": expert_gate, "expert_up": expert_up, "expert_down": expert_down}


epsilon = 1e-06

def rms_scale(values_in, gain_vec):
    return values_in * lax.rsqrt(lax.optimization_barrier(jnp.mean(values_in * values_in, axis=-1, keepdims=True)) + epsilon) * gain_vec

def reference(tokens, mix_gain, query_weight, forget_weight, input_weight, lower_bound, head_gain, out_weight, state, ffn_gain, route_ids, route_weights, expert_gate, expert_up, expert_down):
    batch_size = tokens.shape[0]
    residual = tokens.astype(jnp.float32)
    normed = rms_scale(residual, mix_gain).astype(jnp.bfloat16)
    queries = jnp.dot(normed, query_weight, preferred_element_type=jnp.float32).reshape(batch_size, HEADS, HEAD_DIM)
    forget_pre = jnp.dot(normed, forget_weight, preferred_element_type=jnp.float32)
    fresh_values = jnp.dot(normed, input_weight, preferred_element_type=jnp.float32).reshape(batch_size, HEADS, HEAD_DIM)
    forget = (lower_bound + (1.0 - lower_bound) * jax.nn.sigmoid(forget_pre)).reshape(batch_size, HEADS, HEAD_DIM)
    new_state = forget[..., None] * state + (1.0 - forget)[..., None] * fresh_values[:, :, None, :]
    readout = jnp.einsum('shk,shkv->shv', queries, new_state, precision=lax.Precision.HIGHEST)
    readout = rms_scale(readout, head_gain.reshape(HEADS, HEAD_DIM))
    heads_out = readout.reshape(batch_size, HEADS * HEAD_DIM).astype(jnp.bfloat16)
    group_cols = HEADS * HEAD_DIM // N_TP
    mixer_sum = jnp.zeros((batch_size, D), jnp.float32)
    for group in range(N_TP):
        product = jnp.dot(heads_out[:, group * group_cols:(group + 1) * group_cols], out_weight[group * group_cols:(group + 1) * group_cols], preferred_element_type=jnp.float32).astype(jnp.bfloat16)
        product = lax.optimization_barrier(product)
        mixer_sum = mixer_sum + product.astype(jnp.float32)
    after_mixer = (residual + mixer_sum).astype(jnp.bfloat16)
    ffn_in = rms_scale(after_mixer.astype(jnp.float32), ffn_gain).astype(jnp.bfloat16)
    expert_span = N_EP // EXPERTS
    span_cols = FF_E // expert_span
    gate_full = expert_gate.reshape(EXPERTS, expert_span, D, span_cols).transpose(0, 2, 1, 3).reshape(EXPERTS, D, FF_E)
    up_full = expert_up.reshape(EXPERTS, expert_span, D, span_cols).transpose(0, 2, 1, 3).reshape(EXPERTS, D, FF_E)
    down_full = expert_down.reshape(EXPERTS, FF_E, D)
    pair_count = SEQ_DEV * TOP
    flat_ids = route_ids.reshape(N_EP, pair_count).astype(jnp.int32)
    onehot = (flat_ids[..., None] == jnp.arange(EXPERTS, dtype=jnp.int32)).astype(jnp.int32)
    slot_rank = lax.optimization_barrier(jnp.sum((jnp.cumsum(onehot, axis=1).astype(jnp.int32) - onehot) * onehot, axis=-1)).astype(jnp.int32)
    slot_index = (jnp.arange(N_EP, dtype=jnp.int32)[:, None] * CAP + slot_rank).reshape(-1).astype(jnp.int32)
    expert_index = flat_ids.reshape(-1)
    token_index = (jnp.arange(batch_size * TOP, dtype=jnp.int32) // TOP).astype(jnp.int32)
    slot_table = jnp.full((EXPERTS, N_EP * CAP), batch_size, dtype=jnp.int32).at[expert_index, slot_index].set(token_index)
    padded_rows = jnp.concatenate([ffn_in, jnp.zeros((1, D), jnp.bfloat16)], axis=0)

    def expert_step(inputs):
        gate_w, up_w, down_w, table_row = inputs
        slot_rows = padded_rows[table_row]
        gate_pre = jnp.dot(slot_rows, gate_w, preferred_element_type=jnp.float32)
        up_pre = jnp.dot(slot_rows, up_w, preferred_element_type=jnp.float32)
        hidden = (jax.nn.silu(gate_pre) * up_pre).astype(jnp.bfloat16)
        return jnp.dot(hidden, down_w, preferred_element_type=jnp.float32)
    expert_out = lax.map(expert_step, (gate_full, up_full, down_full, slot_table))
    picked = expert_out[expert_index, slot_index].reshape(batch_size, TOP, D)
    expert_mix = lax.optimization_barrier(jnp.sum(picked * route_weights[:, :, None], axis=1))
    mixed_out = (after_mixer.astype(jnp.float32) + expert_mix).astype(jnp.bfloat16)
    return (mixed_out, new_state)
```

```python
import functools

import jax
import jax.numpy as jnp
from jax import lax
from jax.experimental import pallas as pl
from jax.experimental.pallas import tpu as pltpu
from jax.sharding import PartitionSpec as P


EXPERTS = 8
TOP = 2
LANES = 128
SLOTS = 8


epsilon = 1e-06

NEAR = (0, 1, 2, 4)
GROUP = 4


def xor_pairs(count, mask):
    return [(i, i ^ mask) for i in range(count)]


def aligned(start, size):
    return pl.ds(pl.multiple_of(start, size), size)


def call(kernel, args, outs, scratch=(), flops=3_000_000_000, traffic=100_000, mib=4, hbm=False):
    vmem = pl.BlockSpec(memory_space=pltpu.VMEM)
    return pl.pallas_call(
        kernel,
        out_shape=outs,
        in_specs=[pl.BlockSpec(memory_space=pltpu.HBM) if hbm else vmem] * len(args),
        out_specs=[vmem] * len(outs) if isinstance(outs, list) else vmem,
        scratch_shapes=list(scratch),
        compiler_params=pltpu.CompilerParams(vmem_limit_bytes=mib << 20),
        cost_estimate=pl.CostEstimate(flops=flops, bytes_accessed=traffic, transcendentals=0),
    )(*args)


def prep_kernel(coset, tokens_ref, *refs):
    weight_refs, packed_ref, outs, sems = refs[:3], refs[3], refs[4:-1], refs[-1]
    me = lax.axis_index("ep")
    copies = []

    def start(source, target):
        copy = pltpu.make_async_copy(source, target, sems.at[len(copies)])
        copy.start()
        copies.append(copy)

    for k, ref in enumerate(weight_refs):
        size = ref.shape[1]
        start(ref, packed_ref.at[:, k * size : (k + 1) * size])
    for mask, out in zip(coset, outs):
        for k, near in enumerate(NEAR):
            block = me ^ (mask ^ near)
            start(
                tokens_ref.at[:, aligned(block * LANES, LANES)],
                out.at[:, k * LANES : (k + 1) * LANES],
            )
    for copy in copies:
        copy.wait()


def project_kernel(group, *refs):
    token_refs, gain_ref, weight_refs, outs = (
        refs[:group],
        refs[group],
        refs[group + 1 : group + 5],
        refs[group + 5 :],
    )
    me = lax.axis_index("ep")
    rows = jnp.concatenate([ref[...] for ref in token_refs], axis=0)
    total = None
    for k, near in enumerate(NEAR):
        block = me ^ near
        gain = gain_ref[:, aligned(block * LANES, LANES)]
        scaled = (rows[:, k * LANES : (k + 1) * LANES].astype(jnp.float32) * gain).astype(jnp.bfloat16)
        term = jnp.dot(scaled, weight_refs[k][...], preferred_element_type=jnp.float32)
        total = term if total is None else total + term
    count = token_refs[0].shape[0]
    for m, out in enumerate(outs):
        out[...] = total[m * count : (m + 1) * count].astype(out.dtype)


def state_kernel(group, outer, *refs):
    part_refs = refs[:group]
    tokens_ref, bound_ref, gain_ref, info_ref, state_ref = refs[group : group + 5]
    new_ref = refs[group + 5]
    payloads = refs[group + 6 :]
    count = tokens_ref.shape[0]
    proj = bound_ref.shape[1]
    half = outer // 2

    tokens = tokens_ref[...].astype(jnp.float32)
    scale = lax.rsqrt(jnp.mean(tokens * tokens, axis=-1, keepdims=True) + epsilon)
    for head in range(proj // LANES):

        def pick(which):
            at = slice(which * proj + head * LANES, which * proj + (head + 1) * LANES)
            total = part_refs[0][:, at].astype(jnp.float32)
            for ref in part_refs[1:]:
                total = total + ref[:, at].astype(jnp.float32)
            return total * scale

        cols = slice(head * LANES, (head + 1) * LANES)
        bound = bound_ref[:, cols]
        forget = bound + (1.0 - bound) * jax.nn.sigmoid(pick(0))
        fresh = pick(1)
        query = pick(2)
        forget_t = forget.T
        query_t = query.T
        rows = []
        for s in range(count):
            row = fresh[s : s + 1, :]
            new = row + forget_t[:, s : s + 1] * (state_ref[s, head] - row)
            new_ref[s, head] = new
            rows.append(jnp.sum(query_t[:, s : s + 1] * new, axis=0, keepdims=True))
        readout = jnp.concatenate(rows, axis=0)
        normed = (
            readout
            * lax.rsqrt(jnp.mean(readout * readout, axis=-1, keepdims=True) + epsilon)
            * gain_ref[:, cols]
        ).astype(jnp.bfloat16)
        for out in payloads:
            out[:, cols] = normed

    core = lax.axis_index("tp")
    place = lax.axis_index("ep") % GROUP
    for m, out in enumerate(payloads):
        for a in range(half):
            block = (core * half + a) * GROUP + (place ^ m)
            out[:, proj + a * LANES : proj + (a + 1) * LANES] = tokens_ref[:, aligned(block * LANES, LANES)]
        out[:, proj + half * LANES :] = info_ref[...]


def mix_kernel(outer, *refs):
    payloads = refs[:GROUP]
    weights = refs[GROUP : GROUP + outer]
    own_ref, other_ref, resid_ref, info_ref, heads_ref, part_ref = refs[GROUP + outer :]
    me = lax.axis_index("ep")
    core = lax.axis_index("tp")
    place = me % GROUP
    line = me // GROUP
    half = outer // 2
    count = payloads[0].shape[0]
    proj = weights[0].shape[0]
    for m, ref in enumerate(payloads):
        at = aligned((place ^ m) * count, count)
        heads_ref[at, :] = ref[:, :proj]
        resid_ref[at, :] = ref[:, proj : proj + half * LANES]
        info_ref[at, :] = ref[:, proj + half * LANES :]
    heads = heads_ref[...]
    for m, ref in enumerate(weights):
        product = jnp.dot(heads, ref[...], preferred_element_type=jnp.float32)
        part_ref[:, aligned((line ^ m) * LANES, LANES)] = product.astype(jnp.bfloat16)
    size = half * LANES
    own_ref[...] = part_ref[:, aligned(core * size, size)]
    other_ref[...] = part_ref[:, aligned((1 - core) * size, size)]


def dispatch_kernel(span, own_ref, got_ref, resid_ref, info_ref, out_ref, *rest):
    backs, after_ref = rest[:-1], rest[-1]
    mixer = own_ref[...].astype(jnp.float32) + got_ref[...].astype(jnp.float32)
    after_ref[...] = (resid_ref[...].astype(jnp.float32) + mixer).astype(jnp.bfloat16)
    place = lax.axis_index("ep") % GROUP
    count = after_ref.shape[0] // GROUP
    for m, ref in enumerate(backs):
        ref[...] = after_ref[aligned((place ^ m) * count, count), :]
    after = after_ref[...]
    slots = info_ref[...].astype(jnp.float32).T
    rows = GROUP * SLOTS
    row = lax.broadcasted_iota(jnp.int32, (rows, after.shape[0]), 0)
    col = lax.broadcasted_iota(jnp.int32, (rows, after.shape[0]), 1)
    same = (row // SLOTS) == (col // count)
    slot = (row % SLOTS).astype(jnp.float32)
    for e in range(EXPERTS):
        chosen = same & (slots[e : e + 1, :] == slot)
        select = jnp.where(chosen, 1.0, 0.0).astype(jnp.bfloat16)
        picked = jnp.dot(select, after, preferred_element_type=jnp.float32).astype(jnp.bfloat16)
        for sp in range(span):
            out_ref[e * span + sp] = picked


def expert_kernel(outer, mine_ref, theirs_ref, gain_ref, gate_ref, up_ref, down_ref, own_ref, other_ref, rows_ref, total_ref):
    core = lax.axis_index("tp")
    half = outer // 2
    width = rows_ref.shape[1] // 2
    block = GROUP * SLOTS
    for ref, side in ((mine_ref, core), (theirs_ref, 1 - core)):
        for z in range(outer):
            for q in range(GROUP):
                for a in range(half):
                    at = side * width + (a * GROUP + q) * LANES
                    rows_ref[z * block : (z + 1) * block, aligned(at, LANES)] = ref[
                        z * GROUP + q, :, a * LANES : (a + 1) * LANES
                    ]
    values = rows_ref[...].astype(jnp.float32)
    scale = lax.rsqrt(jnp.mean(values * values, axis=-1, keepdims=True) + epsilon)
    rows = (values * scale * gain_ref[...]).astype(jnp.bfloat16)
    gate = jnp.dot(rows, gate_ref[0], preferred_element_type=jnp.float32)
    up = jnp.dot(rows, up_ref[0], preferred_element_type=jnp.float32)
    hidden = (jax.nn.silu(gate) * up).astype(jnp.bfloat16)
    total_ref[...] = jnp.dot(hidden, down_ref[0], preferred_element_type=jnp.float32).astype(jnp.bfloat16)
    own_ref[...] = total_ref[:, aligned(core * width, width)]
    other_ref[...] = total_ref[:, aligned((1 - core) * width, width)]


def combine_kernel(outer, got_ref, weight_ref, *refs):
    afters, out_ref, base_ref = refs[:GROUP], refs[GROUP], refs[GROUP + 1]
    place = lax.axis_index("ep") % GROUP
    half = outer // 2
    for m, ref in enumerate(afters):
        for a in range(half):
            at = (a * GROUP + (place ^ m)) * LANES
            base_ref[:, aligned(at, LANES)] = ref[:, a * LANES : (a + 1) * LANES].astype(jnp.float32)
    weight = weight_ref[...]
    high = weight.astype(jnp.bfloat16)
    rest = weight - high.astype(jnp.float32)
    middle = rest.astype(jnp.bfloat16)
    low = (rest - middle.astype(jnp.float32)).astype(jnp.bfloat16)
    values = got_ref[...]
    mix = jnp.dot(high, values, preferred_element_type=jnp.float32)
    mix = mix + jnp.dot(middle, values, preferred_element_type=jnp.float32)
    mix = mix + jnp.dot(low, values, preferred_element_type=jnp.float32)
    out_ref[...] = (base_ref[...] + mix).astype(jnp.bfloat16)


def fast_shards(
    tokens,
    mix_gain,
    query_weight,
    forget_weight,
    input_weight,
    lower_bound,
    head_gain,
    out_weight,
    state,
    ffn_gain,
    route_ids,
    route_weights,
    expert_gate,
    expert_up,
    expert_down,
):
    bf16, f32 = jnp.bfloat16, jnp.float32
    ep = lax.axis_size("ep")
    count, width = tokens.shape
    proj = query_weight.shape[1]
    outer = ep // GROUP
    half = outer // 2
    span = ep // EXPERTS
    coset = [h * 8 + b for h in range(ep // 8) for b in (0, 7)]

    def move(value, mask):
        if not mask:
            return value
        return lax.ppermute(value, "ep", xor_pairs(ep, mask))

    def swap(value):
        return lax.ppermute(value, "tp", [(0, 1), (1, 0)])

    def shaped(*shape, dtype=bf16):
        return jax.ShapeDtypeStruct(shape, dtype)

    packed, *sent = call(
        functools.partial(prep_kernel, coset),
        [pltpu.with_memory_space_constraint(a, pltpu.HBM) for a in (tokens, forget_weight, input_weight, query_weight)],
        [shaped(LANES, 3 * proj)] + [shaped(count, len(NEAR) * LANES)] * len(coset),
        scratch=[pltpu.SemaphoreType.DMA((3 + len(coset) * len(NEAR),))],
        hbm=True,
    )
    weights = [move(packed, near) for near in NEAR]
    token_blocks = [move(value, mask) for value, mask in zip(sent, coset)]
    out_weights = [move(out_weight, GROUP * m) for m in range(outer)]

    experts = jnp.arange(EXPERTS, dtype=jnp.int32)
    named = route_ids[:, :, None] == experts
    chosen = jnp.any(named, axis=1)
    before = (jnp.arange(count)[:, None] > jnp.arange(count)[None, :]).astype(f32)
    rank = jnp.sum(before[:, :, None] * chosen.astype(f32)[None, :, :], axis=1)
    slot_of = jnp.where(chosen, rank, 2.0 * SLOTS)
    share = jnp.sum(jnp.where(named, route_weights[:, :, None], 0.0), axis=1)
    info = jnp.pad(slot_of, ((0, 0), (0, LANES - EXPERTS))).astype(bf16)
    places = jnp.arange(SLOTS, dtype=jnp.int32).astype(f32)
    combine = jnp.where(slot_of[:, :, None, None] == places, share[:, :, None, None], 0.0)
    combine = jnp.broadcast_to(combine, (count, EXPERTS, span, SLOTS)).reshape(count, ep * SLOTS)

    parts = call(
        functools.partial(project_kernel, len(coset)),
        (*token_blocks, mix_gain.reshape(1, width), *weights),
        [shaped(count, 3 * proj)] * len(coset),
    )
    parts = [move(value, mask) for value, mask in zip(parts, coset)]

    pay = proj + half * LANES + LANES
    args = (
        *parts,
        tokens,
        lower_bound.reshape(1, proj),
        head_gain.reshape(1, proj),
        info,
        state,
    )
    new_state, *payloads = call(
        functools.partial(state_kernel, len(coset), outer),
        args,
        [shaped(*state.shape, dtype=f32)] + [shaped(count, pay)] * GROUP,
        mib=14,
    )
    payloads = [move(value, m) for m, value in enumerate(payloads)]

    tall = GROUP * count
    own, other, resid, infos = call(
        functools.partial(mix_kernel, outer),
        (*payloads, *out_weights),
        [shaped(tall, half * LANES)] * 3 + [shaped(tall, LANES)],
        scratch=[pltpu.VMEM((tall, proj), bf16), pltpu.VMEM((tall, outer * LANES), bf16)],
    )
    got = swap(other)
    outgoing, *afters = call(
        functools.partial(dispatch_kernel, span),
        (own, got, resid, infos),
        [shaped(ep, GROUP * SLOTS, half * LANES)] + [shaped(count, half * LANES)] * GROUP,
        scratch=[pltpu.VMEM((tall, half * LANES), bf16)],
    )
    slot_rows = lax.all_to_all(outgoing, "ep", split_axis=0, concat_axis=0, tiled=True)
    afters = [move(value, m) for m, value in enumerate(afters)]
    other_rows = swap(slot_rows)

    total_rows = ep * SLOTS
    mine, theirs = call(
        functools.partial(expert_kernel, outer),
        (slot_rows, other_rows, ffn_gain.reshape(1, width), expert_gate, expert_up, expert_down),
        [shaped(total_rows, width // 2)] * 2,
        scratch=[pltpu.VMEM((total_rows, width), bf16), pltpu.VMEM((total_rows, width), bf16)],
        mib=24,
    )
    reduced = (mine.astype(f32) + swap(theirs).astype(f32)).astype(bf16)
    returned = lax.all_to_all(
        reduced.reshape(ep, SLOTS, width // 2), "ep", split_axis=0, concat_axis=0, tiled=True
    )
    mixed_out = call(
        functools.partial(combine_kernel, outer),
        (returned.reshape(total_rows, width // 2), combine, *afters),
        shaped(count, width // 2),
        scratch=[pltpu.VMEM((count, width // 2), f32)],
    )
    return (mixed_out, new_state)


def rms_scale(values_in, gain_vec):
    return (
        values_in
        * lax.rsqrt(jnp.mean(values_in * values_in, axis=-1, keepdims=True) + epsilon)
        * gain_vec
    )


def slot_ranks(block_ids, expert_count):
    onehot = (block_ids[..., None] == jnp.arange(expert_count, dtype=jnp.int32)).astype(jnp.int32)
    before = jnp.cumsum(onehot, axis=1) - onehot
    return jnp.sum(before * onehot, axis=-1)


def general_shards(
    tokens,
    mix_gain,
    query_weight,
    forget_weight,
    input_weight,
    lower_bound,
    head_gain,
    out_weight,
    state,
    ffn_gain,
    route_ids,
    route_weights,
    expert_gate,
    expert_up,
    expert_down,
):
    seq_dev = tokens.shape[0]
    model_width = tokens.shape[1]
    ep_count = lax.axis_size("ep")
    residual = tokens.astype(jnp.float32)
    normed = rms_scale(residual, mix_gain).astype(jnp.bfloat16)
    head_count = state.shape[1]
    head_size = state.shape[2]
    proj_width = query_weight.shape[1]
    pieces = (
        lax.all_gather(query_weight, "ep", axis=0, tiled=True),
        lax.all_gather(forget_weight, "ep", axis=0, tiled=True),
        lax.all_gather(input_weight, "ep", axis=0, tiled=True),
    )
    queries, forget_pre, fresh_values = tuple(
        (jnp.dot(normed, weight_rows, preferred_element_type=jnp.float32) for weight_rows in pieces)
    )
    forget = (lower_bound + (1.0 - lower_bound) * jax.nn.sigmoid(forget_pre)).reshape(
        seq_dev, head_count, head_size
    )
    queries = queries.reshape(seq_dev, head_count, head_size)
    fresh_values = fresh_values.reshape(seq_dev, head_count, head_size)
    new_state = forget[..., None] * state + (1.0 - forget)[..., None] * fresh_values[:, :, None, :]
    readout = jnp.einsum("shk,shkv->shv", queries, new_state, precision=lax.Precision.HIGHEST)
    readout = rms_scale(readout, head_gain.reshape(head_count, head_size))
    heads_out = readout.reshape(seq_dev, proj_width).astype(jnp.bfloat16)
    partial_mix = jnp.dot(
        heads_out,
        lax.all_gather(out_weight, "ep", axis=1, tiled=True),
        preferred_element_type=jnp.float32,
    )
    mixer_sum = lax.psum(partial_mix.astype(jnp.bfloat16), "tp").astype(jnp.float32)
    after_mixer = (residual + mixer_sum).astype(jnp.bfloat16)
    ffn_in = rms_scale(after_mixer.astype(jnp.float32), ffn_gain).astype(jnp.bfloat16)
    capacity = 3 * seq_dev // 8
    expert_span = ep_count // EXPERTS
    half_width = model_width // lax.axis_size("tp")
    own_columns = lax.dynamic_slice_in_dim(
        after_mixer, lax.axis_index("tp") * half_width, half_width, 1
    ).astype(jnp.float32)
    gate_slice = expert_gate[0]
    up_slice = expert_up[0]
    down_slice = expert_down[0]
    slot_iota = jnp.arange(capacity, dtype=jnp.int32)
    own_rank = slot_ranks(route_ids.reshape(1, seq_dev * TOP), EXPERTS).reshape(seq_dev, TOP)
    expert_iota = jnp.arange(EXPERTS, dtype=jnp.int32)
    chosen = (route_ids[:, :, None, None] == expert_iota[None, None, :, None]) & (
        own_rank[:, :, None, None] == slot_iota[None, None, None, :]
    )
    dispatch = jnp.any(chosen, axis=1).astype(jnp.bfloat16)
    combine = jnp.sum(chosen.astype(jnp.float32) * route_weights[:, :, None, None], axis=1)
    outgoing = jnp.einsum(
        "tec,td->ecd", dispatch, ffn_in, preferred_element_type=jnp.float32
    ).astype(jnp.bfloat16)
    outgoing = jnp.broadcast_to(
        outgoing[:, None], (EXPERTS, expert_span, capacity, model_width)
    ).reshape(ep_count, capacity, model_width)
    slot_rows = lax.all_to_all(outgoing, "ep", split_axis=0, concat_axis=0, tiled=True)
    gate_pre = jnp.einsum(
        "...d,df->...f", slot_rows, gate_slice, preferred_element_type=jnp.float32
    )
    up_pre = jnp.einsum("...d,df->...f", slot_rows, up_slice, preferred_element_type=jnp.float32)
    hidden = (jax.nn.silu(gate_pre) * up_pre).astype(jnp.bfloat16)
    partial_out = jnp.einsum(
        "...f,fd->...d", hidden, down_slice, preferred_element_type=jnp.float32
    )
    reduced = lax.psum_scatter(
        partial_out.astype(jnp.bfloat16), "tp", scatter_dimension=2, tiled=True
    ).astype(jnp.float32)
    returned = lax.all_to_all(
        reduced.astype(jnp.bfloat16), "ep", split_axis=0, concat_axis=0, tiled=True
    ).astype(reduced.dtype)
    expert_out = jnp.sum(returned.reshape(EXPERTS, expert_span, capacity, half_width), axis=1)
    expert_mix = jnp.einsum("tec,ecd->td", combine, expert_out, precision=lax.Precision.HIGHEST)
    mixed_out = (own_columns + expert_mix).astype(jnp.bfloat16)
    return (mixed_out, new_state)


def shards(*args):
    tokens, query_weight, state = args[0], args[2], args[8]
    ep, tp = lax.axis_size("ep"), lax.axis_size("tp")
    fits = (
        tp == 2
        and ep % 8 == 0
        and ep % EXPERTS == 0
        and tokens.shape[0] % 16 == 0
        and 3 * tokens.shape[0] // 8 <= SLOTS
        and tokens.shape[1] == ep * LANES
        and query_weight.shape[0] == LANES
        and state.shape[2:] == (LANES, LANES)
        and args[12].shape[2] % (4 * LANES) == 0
    )
    if not fits:
        return general_shards(*args)
    return fast_shards(*args)


def solution(mesh):
    return jax.shard_map(
        shards,
        mesh=mesh,
        in_specs=(
            P("ep", None),
            P(),
            P("ep", "tp"),
            P("ep", "tp"),
            P("ep", "tp"),
            P("tp"),
            P("tp"),
            P("tp", "ep"),
            P("ep", "tp", None, None),
            P(),
            P("ep", None),
            P("ep", None),
            P("ep", None, "tp"),
            P("ep", None, "tp"),
            P("ep", "tp", None),
        ),
        out_specs=(P("ep", "tp"), P("ep", "tp", None, None)),
        check_vma=False,
    )
```

```python
import functools

import jax
import jax.numpy as jnp
from jax import lax
from jax.experimental import pallas as pl
from jax.experimental.pallas import tpu as pltpu
from jax.sharding import PartitionSpec as P


EXPERTS = 8
TOP = 2
LANES = 128


epsilon = 1e-06

NEAR = (0, 1, 2, 4)
GROUP = 4


def xor_pairs(count, mask):
    return [(i, i ^ mask) for i in range(count)]


def aligned(start, size):
    return pl.ds(pl.multiple_of(start, size), size)


def call(kernel, args, outs, scratch=(), flops=3_000_000_000, traffic=100_000, mib=4, hbm=False):
    vmem = pl.BlockSpec(memory_space=pltpu.VMEM)
    return pl.pallas_call(
        kernel,
        out_shape=outs,
        in_specs=[pl.BlockSpec(memory_space=pltpu.HBM) if hbm else vmem] * len(args),
        out_specs=[vmem] * len(outs) if isinstance(outs, list) else vmem,
        scratch_shapes=list(scratch),
        compiler_params=pltpu.CompilerParams(vmem_limit_bytes=mib << 20),
        cost_estimate=pl.CostEstimate(flops=flops, bytes_accessed=traffic, transcendentals=0),
    )(*args)


def thirds(values):
    high = values.astype(jnp.bfloat16)
    rest = values - high.astype(jnp.float32)
    middle = rest.astype(jnp.bfloat16)
    low = (rest - middle.astype(jnp.float32)).astype(jnp.bfloat16)
    return high, middle, low


def spreader(count):
    shape = (3 * count, count * LANES)
    row = lax.broadcasted_iota(jnp.int32, shape, 0) % count
    col = lax.broadcasted_iota(jnp.int32, shape, 1) // LANES
    return jnp.where(row == col, 1.0, 0.0).astype(jnp.bfloat16)


def spread(values, matrix):
    return lax.dot_general(
        jnp.concatenate([part.astype(jnp.float32) for part in thirds(values)], axis=0).astype(jnp.bfloat16),
        matrix,
        (((0,), (0,)), ((), ())),
        preferred_element_type=jnp.float32,
    )


def prep_kernel(coset, tokens_ref, *refs):
    weight_refs, packed_ref, outs, sems = refs[:3], refs[3], refs[4:-1], refs[-1]
    me = lax.axis_index("ep")
    copies = []

    def start(source, target):
        copy = pltpu.make_async_copy(source, target, sems.at[len(copies)])
        copy.start()
        copies.append(copy)

    for k, ref in enumerate(weight_refs):
        size = ref.shape[1]
        start(ref, packed_ref.at[:, k * size : (k + 1) * size])
    for mask, out in zip(coset, outs):
        for k, near in enumerate(NEAR):
            block = me ^ (mask ^ near)
            start(
                tokens_ref.at[:, aligned(block * LANES, LANES)],
                out.at[:, k * LANES : (k + 1) * LANES],
            )
    for copy in copies:
        copy.wait()


def route_kernel(cap, span, ids_ref, weights_ref, info_ref, combine_ref):
    count = ids_ref.shape[0]
    ids, weights = ids_ref[...], weights_ref[...]
    lane = lax.broadcasted_iota(jnp.int32, (count, LANES), 1)
    picks = [ids[:, k : k + 1] == lane for k in range(TOP)]
    chosen = functools.reduce(jnp.logical_or, picks)
    earlier = lax.broadcasted_iota(jnp.int32, (count, count), 0) > lax.broadcasted_iota(
        jnp.int32, (count, count), 1
    )
    rank = jnp.dot(
        jnp.where(earlier, 1.0, 0.0).astype(jnp.bfloat16),
        jnp.where(chosen, 1.0, 0.0).astype(jnp.bfloat16),
        preferred_element_type=jnp.float32,
    )
    info_ref[...] = jnp.where(chosen, rank, 2.0 * count).astype(jnp.bfloat16)
    column = lax.broadcasted_iota(jnp.int32, combine_ref.shape, 1)
    expert = column // (span * GROUP * cap)
    place = (column % cap).astype(jnp.float32)
    total = jnp.zeros(combine_ref.shape, jnp.float32)
    for k in range(TOP):
        own = jnp.sum(jnp.where(picks[k], rank, 0.0), axis=-1, keepdims=True)
        hit = (ids[:, k : k + 1] == expert) & (own == place)
        total = total + jnp.where(hit, weights[:, k : k + 1], 0.0)
    combine_ref[...] = total


def project_kernel(group, *refs):
    token_refs, gain_ref, weight_refs, outs = (
        refs[:group],
        refs[group],
        refs[group + 1 : group + 5],
        refs[group + 5 :],
    )
    me = lax.axis_index("ep")
    rows = jnp.concatenate([ref[...] for ref in token_refs], axis=0)
    total = None
    for k, near in enumerate(NEAR):
        block = me ^ near
        gain = gain_ref[:, aligned(block * LANES, LANES)]
        scaled = (rows[:, k * LANES : (k + 1) * LANES].astype(jnp.float32) * gain).astype(jnp.bfloat16)
        term = jnp.dot(scaled, weight_refs[k][...], preferred_element_type=jnp.float32)
        total = term if total is None else total + term
    count = token_refs[0].shape[0]
    for m, out in enumerate(outs):
        out[...] = total[m * count : (m + 1) * count].astype(out.dtype)


def readout_kernel(group, outer, *refs):
    part_refs = refs[:group]
    tokens_ref, bound_ref, gain_ref, info_ref, state_ref = refs[group : group + 5]
    forget_ref, fresh_ref = refs[group + 5 : group + 7]
    payloads = refs[group + 7 :]
    count = tokens_ref.shape[0]
    proj = bound_ref.shape[1]
    half = outer // 2

    tokens = tokens_ref[...].astype(jnp.float32)
    scale = lax.rsqrt(jnp.mean(tokens * tokens, axis=-1, keepdims=True) + epsilon)
    matrix = spreader(count)
    for head in range(proj // LANES):

        def pick(which):
            at = slice(which * proj + head * LANES, which * proj + (head + 1) * LANES)
            total = part_refs[0][:, at].astype(jnp.float32)
            for ref in part_refs[1:]:
                total = total + ref[:, at].astype(jnp.float32)
            return total * scale

        cols = slice(head * LANES, (head + 1) * LANES)
        bound = bound_ref[:, cols]
        forget = bound + (1.0 - bound) * jax.nn.sigmoid(pick(0))
        fresh = pick(1)
        query = pick(2)
        forget_ref[:, cols] = forget
        fresh_ref[:, cols] = fresh
        kept = spread(query * forget, matrix)
        rows = [
            jnp.sum(kept[:, s * LANES : (s + 1) * LANES] * state_ref[s, head], axis=0, keepdims=True)
            for s in range(count)
        ]
        added = jnp.sum(query * (1.0 - forget), axis=-1, keepdims=True) * fresh
        readout = jnp.concatenate(rows, axis=0) + added
        normed = (
            readout
            * lax.rsqrt(jnp.mean(readout * readout, axis=-1, keepdims=True) + epsilon)
            * gain_ref[:, cols]
        ).astype(jnp.bfloat16)
        for out in payloads:
            out[:, cols] = normed

    core = lax.axis_index("tp")
    place = lax.axis_index("ep") % GROUP
    for m, out in enumerate(payloads):
        for a in range(half):
            block = (core * half + a) * GROUP + (place ^ m)
            out[:, proj + a * LANES : proj + (a + 1) * LANES] = tokens_ref[:, aligned(block * LANES, LANES)]
        out[:, proj + half * LANES :] = info_ref[...]


def update_kernel(forget_ref, fresh_ref, state_ref, new_ref):
    count = forget_ref.shape[0]
    kept = spread(forget_ref[...], spreader(count))
    for s in range(count):
        keep = kept[:, s * LANES : (s + 1) * LANES]
        new_ref[s, 0] = keep * state_ref[s, 0] + (1.0 - keep) * fresh_ref[s : s + 1, :]


def mix_kernel(outer, *refs):
    payloads = refs[:GROUP]
    weights = refs[GROUP : GROUP + outer]
    own_ref, other_ref, resid_ref, info_ref, heads_ref, part_ref = refs[GROUP + outer :]
    me = lax.axis_index("ep")
    core = lax.axis_index("tp")
    place = me % GROUP
    line = me // GROUP
    half = outer // 2
    count = payloads[0].shape[0]
    proj = weights[0].shape[0]
    for m, ref in enumerate(payloads):
        at = aligned((place ^ m) * count, count)
        heads_ref[at, :] = ref[:, :proj]
        resid_ref[at, :] = ref[:, proj : proj + half * LANES]
        info_ref[at, :] = ref[:, proj + half * LANES :]
    heads = heads_ref[...]
    for m, ref in enumerate(weights):
        product = jnp.dot(heads, ref[...], preferred_element_type=jnp.float32)
        part_ref[:, aligned((line ^ m) * LANES, LANES)] = product.astype(jnp.bfloat16)
    size = half * LANES
    own_ref[...] = part_ref[:, aligned(core * size, size)]
    other_ref[...] = part_ref[:, aligned((1 - core) * size, size)]


def dispatch_kernel(span, own_ref, got_ref, resid_ref, info_ref, out_ref, *rest):
    backs, after_ref = rest[:-1], rest[-1]
    mixer = own_ref[...].astype(jnp.float32) + got_ref[...].astype(jnp.float32)
    after_ref[...] = (resid_ref[...].astype(jnp.float32) + mixer).astype(jnp.bfloat16)
    place = lax.axis_index("ep") % GROUP
    count = after_ref.shape[0] // GROUP
    for m, ref in enumerate(backs):
        ref[...] = after_ref[aligned((place ^ m) * count, count), :]
    after = after_ref[...]
    slots = info_ref[...].astype(jnp.float32).T
    rows = out_ref.shape[1]
    cap = rows // GROUP
    row = lax.broadcasted_iota(jnp.int32, (rows, after.shape[0]), 0)
    col = lax.broadcasted_iota(jnp.int32, (rows, after.shape[0]), 1)
    same = (row // cap) == (col // count)
    slot = (row % cap).astype(jnp.float32)
    for e in range(EXPERTS):
        chosen = same & (slots[e : e + 1, :] == slot)
        select = jnp.where(chosen, 1.0, 0.0).astype(jnp.bfloat16)
        picked = jnp.dot(select, after, preferred_element_type=jnp.float32).astype(jnp.bfloat16)
        for sp in range(span):
            out_ref[e * span + sp] = picked


def expert_kernel(outer, mine_ref, theirs_ref, gain_ref, gate_ref, up_ref, down_ref, own_ref, other_ref, rows_ref, total_ref):
    core = lax.axis_index("tp")
    half = outer // 2
    total_rows, width = rows_ref.shape[0], rows_ref.shape[1] // 2
    block = mine_ref.shape[1]
    cap = block // GROUP
    for ref, side in ((mine_ref, core), (theirs_ref, 1 - core)):
        for z in range(outer):
            for q in range(GROUP):
                for a in range(half):
                    at = side * width + (a * GROUP + q) * LANES
                    rows_ref[z * block : (z + 1) * block, aligned(at, LANES)] = ref[
                        z * GROUP + q, :, a * LANES : (a + 1) * LANES
                    ].astype(jnp.float32)
    values = rows_ref[...]
    scale = lax.rsqrt(jnp.mean(values * values, axis=-1, keepdims=True) + epsilon)
    rows = (values * scale * gain_ref[...]).astype(jnp.bfloat16)
    gate = jnp.dot(rows, gate_ref[0], preferred_element_type=jnp.float32)
    up = jnp.dot(rows, up_ref[0], preferred_element_type=jnp.float32)
    hidden = (jax.nn.silu(gate) * up).astype(jnp.bfloat16)
    total_ref[...] = jnp.dot(hidden, down_ref[0], preferred_element_type=jnp.float32).astype(jnp.bfloat16)
    part = width // GROUP
    tall = own_ref.shape[0]
    row = lax.broadcasted_iota(jnp.int32, (tall, total_rows), 0)
    col = lax.broadcasted_iota(jnp.int32, (tall, total_rows), 1)
    source = (row // block) * cap + row % cap
    piece = (row % block) // cap
    selects = [
        jnp.where((source == col) & (piece == k), 1.0, 0.0).astype(jnp.bfloat16) for k in range(GROUP)
    ]
    for ref, side in ((other_ref, 1 - core), (own_ref, core)):
        packed = None
        for k, select in enumerate(selects):
            values = total_ref[:, aligned(side * width + k * part, part)]
            term = jnp.dot(select, values, preferred_element_type=jnp.float32)
            packed = term if packed is None else packed + term
        ref[...] = packed.astype(jnp.bfloat16)


def combine_kernel(outer, cap, got_ref, weight_ref, *refs):
    afters, out_ref, base_ref = refs[:GROUP], refs[GROUP], refs[GROUP + 1]
    place = lax.axis_index("ep") % GROUP
    half = outer // 2
    for m, ref in enumerate(afters):
        for a in range(half):
            at = (a * GROUP + (place ^ m)) * LANES
            base_ref[:, aligned(at, LANES)] = ref[:, a * LANES : (a + 1) * LANES].astype(jnp.float32)
    weight = weight_ref[...]
    values = got_ref[...]
    _, part = values.shape
    block = GROUP * cap
    count = weight.shape[0]
    piece = (lax.broadcasted_iota(jnp.int32, weight.shape, 1) % block) // cap
    parts = thirds(weight)
    for k in range(GROUP):
        split = [jnp.where(piece == k, w.astype(jnp.float32), 0.0) for w in parts]
        stacked = jnp.concatenate(split, axis=0).astype(jnp.bfloat16)
        mix = jnp.dot(stacked, values, preferred_element_type=jnp.float32)
        mix = mix[:count] + mix[count : 2 * count] + mix[2 * count :]
        at = slice(k * part, (k + 1) * part)
        out_ref[:, at] = (base_ref[:, at] + mix).astype(jnp.bfloat16)


def fast_shards(
    tokens,
    mix_gain,
    query_weight,
    forget_weight,
    input_weight,
    lower_bound,
    head_gain,
    out_weight,
    state,
    ffn_gain,
    route_ids,
    route_weights,
    expert_gate,
    expert_up,
    expert_down,
):
    bf16, f32 = jnp.bfloat16, jnp.float32
    ep = lax.axis_size("ep")
    count, width = tokens.shape
    heads, size = state.shape[1], state.shape[2]
    proj = query_weight.shape[1]
    outer = ep // GROUP
    half = outer // 2
    span = ep // EXPERTS
    coset = [h * 8 + b for h in range(ep // 8) for b in (0, 7)]

    def move(value, mask):
        if not mask:
            return value
        return lax.ppermute(value, "ep", xor_pairs(ep, mask))

    def swap(value):
        return lax.ppermute(value, "tp", [(0, 1), (1, 0)])

    def shaped(*shape, dtype=bf16):
        return jax.ShapeDtypeStruct(shape, dtype)

    packed, *sent = call(
        functools.partial(prep_kernel, coset),
        [pltpu.with_memory_space_constraint(a, pltpu.HBM) for a in (tokens, forget_weight, input_weight, query_weight)],
        [shaped(LANES, 3 * proj)] + [shaped(count, len(NEAR) * LANES)] * len(coset),
        scratch=[pltpu.SemaphoreType.DMA((3 + len(coset) * len(NEAR),))],
        hbm=True,
    )
    weights = [move(packed, near) for near in NEAR]
    token_blocks = [move(value, mask) for value, mask in zip(sent, coset)]
    out_weights = [move(out_weight, GROUP * m) for m in range(outer)]

    cap = 3 * count // 8
    rows_out = GROUP * cap
    info, combine = call(
        functools.partial(route_kernel, cap, span),
        (route_ids, route_weights),
        [shaped(count, LANES), shaped(count, ep * rows_out, dtype=f32)],
    )

    parts = call(
        functools.partial(project_kernel, len(coset)),
        (*token_blocks, mix_gain.reshape(1, width), *weights),
        [shaped(count, 3 * proj)] * len(coset),
    )
    parts = [move(value, mask) for value, mask in zip(parts, coset)]

    pay = proj + half * LANES + LANES
    args = (
        *parts,
        tokens,
        lower_bound.reshape(1, proj),
        head_gain.reshape(1, proj),
        info,
        state,
    )
    forget, fresh, *payloads = call(
        functools.partial(readout_kernel, len(coset), outer),
        args,
        [shaped(count, proj, dtype=f32)] * 2 + [shaped(count, pay)] * GROUP,
    )
    payloads = [move(value, m) for m, value in enumerate(payloads)]

    tall = GROUP * count
    own, other, resid, infos = call(
        functools.partial(mix_kernel, outer),
        (*payloads, *out_weights),
        [shaped(tall, half * LANES)] * 3 + [shaped(tall, LANES)],
        scratch=[pltpu.VMEM((tall, proj), bf16), pltpu.VMEM((tall, outer * LANES), bf16)],
    )
    got = swap(other)
    outgoing, *afters = call(
        functools.partial(dispatch_kernel, span),
        (own, got, resid, infos),
        [shaped(ep, rows_out, half * LANES)] + [shaped(count, half * LANES)] * GROUP,
        scratch=[pltpu.VMEM((tall, half * LANES), bf16)],
    )
    slot_rows = lax.all_to_all(outgoing, "ep", split_axis=0, concat_axis=0, tiled=True)
    afters = [move(value, m) for m, value in enumerate(afters)]
    other_rows = swap(slot_rows)

    total_rows = ep * cap
    tall = ep * rows_out
    part = width // 2 // GROUP
    mine, theirs = call(
        functools.partial(expert_kernel, outer),
        (slot_rows, other_rows, ffn_gain.reshape(1, width), expert_gate, expert_up, expert_down),
        [shaped(tall, part)] * 2,
        scratch=[pltpu.VMEM((total_rows, width), f32), pltpu.VMEM((total_rows, width), bf16)],
        mib=24,
    )
    reduced = (mine.astype(f32) + swap(theirs).astype(f32)).astype(bf16)
    returned = lax.all_to_all(
        reduced.reshape(ep, rows_out, part), "ep", split_axis=0, concat_axis=0, tiled=True
    )
    block = pl.BlockSpec((count, 1, size, size), lambda h: (0, h, 0, 0))
    column = pl.BlockSpec((count, size), lambda h: (0, h))
    new_state = pl.pallas_call(
        update_kernel,
        out_shape=shaped(*state.shape, dtype=f32),
        grid=(heads,),
        in_specs=[column, column, block],
        out_specs=block,
        compiler_params=pltpu.CompilerParams(vmem_limit_bytes=12 << 20),
        cost_estimate=pl.CostEstimate(flops=3_000_000_000, bytes_accessed=8_000_000, transcendentals=0),
    )(forget, fresh, pltpu.with_memory_space_constraint(state, pltpu.HBM))
    mixed_out = call(
        functools.partial(combine_kernel, outer, cap),
        (returned.reshape(tall, part), combine, *afters),
        shaped(count, width // 2),
        scratch=[pltpu.VMEM((count, width // 2), f32)],
    )
    return (mixed_out, new_state)


def rms_scale(values_in, gain_vec):
    return (
        values_in
        * lax.rsqrt(jnp.mean(values_in * values_in, axis=-1, keepdims=True) + epsilon)
        * gain_vec
    )


def slot_ranks(block_ids, expert_count):
    onehot = (block_ids[..., None] == jnp.arange(expert_count, dtype=jnp.int32)).astype(jnp.int32)
    before = jnp.cumsum(onehot, axis=1) - onehot
    return jnp.sum(before * onehot, axis=-1)


def general_shards(
    tokens,
    mix_gain,
    query_weight,
    forget_weight,
    input_weight,
    lower_bound,
    head_gain,
    out_weight,
    state,
    ffn_gain,
    route_ids,
    route_weights,
    expert_gate,
    expert_up,
    expert_down,
):
    seq_dev = tokens.shape[0]
    model_width = tokens.shape[1]
    ep_count = lax.axis_size("ep")
    residual = tokens.astype(jnp.float32)
    normed = rms_scale(residual, mix_gain).astype(jnp.bfloat16)
    head_count = state.shape[1]
    head_size = state.shape[2]
    proj_width = query_weight.shape[1]
    pieces = (
        lax.all_gather(query_weight, "ep", axis=0, tiled=True),
        lax.all_gather(forget_weight, "ep", axis=0, tiled=True),
        lax.all_gather(input_weight, "ep", axis=0, tiled=True),
    )
    queries, forget_pre, fresh_values = tuple(
        (jnp.dot(normed, weight_rows, preferred_element_type=jnp.float32) for weight_rows in pieces)
    )
    forget = (lower_bound + (1.0 - lower_bound) * jax.nn.sigmoid(forget_pre)).reshape(
        seq_dev, head_count, head_size
    )
    queries = queries.reshape(seq_dev, head_count, head_size)
    fresh_values = fresh_values.reshape(seq_dev, head_count, head_size)
    new_state = forget[..., None] * state + (1.0 - forget)[..., None] * fresh_values[:, :, None, :]
    readout = jnp.einsum("shk,shkv->shv", queries, new_state, precision=lax.Precision.HIGHEST)
    readout = rms_scale(readout, head_gain.reshape(head_count, head_size))
    heads_out = readout.reshape(seq_dev, proj_width).astype(jnp.bfloat16)
    partial_mix = jnp.dot(
        heads_out,
        lax.all_gather(out_weight, "ep", axis=1, tiled=True),
        preferred_element_type=jnp.float32,
    )
    mixer_sum = lax.psum(partial_mix.astype(jnp.bfloat16), "tp").astype(jnp.float32)
    after_mixer = (residual + mixer_sum).astype(jnp.bfloat16)
    ffn_in = rms_scale(after_mixer.astype(jnp.float32), ffn_gain).astype(jnp.bfloat16)
    capacity = 3 * seq_dev // 8
    expert_span = ep_count // EXPERTS
    half_width = model_width // lax.axis_size("tp")
    own_columns = lax.dynamic_slice_in_dim(
        after_mixer, lax.axis_index("tp") * half_width, half_width, 1
    ).astype(jnp.float32)
    gate_slice = expert_gate[0]
    up_slice = expert_up[0]
    down_slice = expert_down[0]
    slot_iota = jnp.arange(capacity, dtype=jnp.int32)
    own_rank = slot_ranks(route_ids.reshape(1, seq_dev * TOP), EXPERTS).reshape(seq_dev, TOP)
    expert_iota = jnp.arange(EXPERTS, dtype=jnp.int32)
    chosen = (route_ids[:, :, None, None] == expert_iota[None, None, :, None]) & (
        own_rank[:, :, None, None] == slot_iota[None, None, None, :]
    )
    dispatch = jnp.any(chosen, axis=1).astype(jnp.bfloat16)
    combine = jnp.sum(chosen.astype(jnp.float32) * route_weights[:, :, None, None], axis=1)
    outgoing = jnp.einsum(
        "tec,td->ecd", dispatch, ffn_in, preferred_element_type=jnp.float32
    ).astype(jnp.bfloat16)
    outgoing = jnp.broadcast_to(
        outgoing[:, None], (EXPERTS, expert_span, capacity, model_width)
    ).reshape(ep_count, capacity, model_width)
    slot_rows = lax.all_to_all(outgoing, "ep", split_axis=0, concat_axis=0, tiled=True)
    gate_pre = jnp.einsum(
        "...d,df->...f", slot_rows, gate_slice, preferred_element_type=jnp.float32
    )
    up_pre = jnp.einsum("...d,df->...f", slot_rows, up_slice, preferred_element_type=jnp.float32)
    hidden = (jax.nn.silu(gate_pre) * up_pre).astype(jnp.bfloat16)
    partial_out = jnp.einsum(
        "...f,fd->...d", hidden, down_slice, preferred_element_type=jnp.float32
    )
    reduced = lax.psum_scatter(
        partial_out.astype(jnp.bfloat16), "tp", scatter_dimension=2, tiled=True
    ).astype(jnp.float32)
    returned = lax.all_to_all(
        reduced.astype(jnp.bfloat16), "ep", split_axis=0, concat_axis=0, tiled=True
    ).astype(reduced.dtype)
    expert_out = jnp.sum(returned.reshape(EXPERTS, expert_span, capacity, half_width), axis=1)
    expert_mix = jnp.einsum("tec,ecd->td", combine, expert_out, precision=lax.Precision.HIGHEST)
    mixed_out = (own_columns + expert_mix).astype(jnp.bfloat16)
    return (mixed_out, new_state)


def shards(*args):
    tokens, query_weight, state = args[0], args[2], args[8]
    ep, tp = lax.axis_size("ep"), lax.axis_size("tp")
    fits = (
        tp == 2
        and ep % 8 == 0
        and ep % EXPERTS == 0
        and tokens.shape[0] % 16 == 0
        and 3 * tokens.shape[0] // 8 % 2 == 0
        and tokens.shape[1] == ep * LANES
        and query_weight.shape[0] == LANES
        and state.shape[2:] == (LANES, LANES)
        and args[12].shape[2] % (4 * LANES) == 0
    )
    if not fits:
        return general_shards(*args)
    return fast_shards(*args)


def solution(mesh):
    return jax.shard_map(
        shards,
        mesh=mesh,
        in_specs=(
            P("ep", None),
            P(),
            P("ep", "tp"),
            P("ep", "tp"),
            P("ep", "tp"),
            P("tp"),
            P("tp"),
            P("tp", "ep"),
            P("ep", "tp", None, None),
            P(),
            P("ep", None),
            P("ep", None),
            P("ep", None, "tp"),
            P("ep", None, "tp"),
            P("ep", "tp", None),
        ),
        out_specs=(P("ep", "tp"), P("ep", "tp", None, None)),
        check_vma=False,
    )
```

```python
import functools

import jax
import jax.numpy as jnp
from jax import lax
from jax.experimental import pallas as pl
from jax.experimental.pallas import tpu as pltpu
from jax.sharding import PartitionSpec as P


EXPERTS = 8
TOP = 2
LANES = 128


epsilon = 1e-06

NEAR = (0, 1, 2, 4)
GROUP = 4


def xor_pairs(count, mask):
    return [(i, i ^ mask) for i in range(count)]


def aligned(start, size):
    return pl.ds(pl.multiple_of(start, size), size)


def call(kernel, args, outs, scratch=(), flops=3_000_000_000, traffic=100_000, mib=4, hbm=False):
    vmem = pl.BlockSpec(memory_space=pltpu.VMEM)
    return pl.pallas_call(
        kernel,
        out_shape=outs,
        in_specs=[pl.BlockSpec(memory_space=pltpu.HBM) if hbm else vmem] * len(args),
        out_specs=[vmem] * len(outs) if isinstance(outs, list) else vmem,
        scratch_shapes=list(scratch),
        compiler_params=pltpu.CompilerParams(vmem_limit_bytes=mib << 20),
        cost_estimate=pl.CostEstimate(flops=flops, bytes_accessed=traffic, transcendentals=0),
    )(*args)


def thirds(values):
    high = values.astype(jnp.bfloat16)
    rest = values - high.astype(jnp.float32)
    middle = rest.astype(jnp.bfloat16)
    low = (rest - middle.astype(jnp.float32)).astype(jnp.bfloat16)
    return high, middle, low


def spreader(count):
    shape = (3 * count, count * LANES)
    row = lax.broadcasted_iota(jnp.int32, shape, 0) % count
    col = lax.broadcasted_iota(jnp.int32, shape, 1) // LANES
    return jnp.where(row == col, 1.0, 0.0).astype(jnp.bfloat16)


def spread(values, matrix):
    return lax.dot_general(
        jnp.concatenate([part.astype(jnp.float32) for part in thirds(values)], axis=0).astype(jnp.bfloat16),
        matrix,
        (((0,), (0,)), ((), ())),
        preferred_element_type=jnp.float32,
    )


def prep_kernel(coset, tokens_ref, *refs):
    weight_refs, packed_ref, outs, sems = refs[:3], refs[3], refs[4:-1], refs[-1]
    me = lax.axis_index("ep")
    copies = []

    def start(source, target):
        copy = pltpu.make_async_copy(source, target, sems.at[len(copies)])
        copy.start()
        copies.append(copy)

    for k, ref in enumerate(weight_refs):
        size = ref.shape[1]
        start(ref, packed_ref.at[:, k * size : (k + 1) * size])
    for mask, out in zip(coset, outs):
        for k, near in enumerate(NEAR):
            block = me ^ (mask ^ near)
            start(
                tokens_ref.at[:, aligned(block * LANES, LANES)],
                out.at[:, k * LANES : (k + 1) * LANES],
            )
    for copy in copies:
        copy.wait()


def route_kernel(cap, span, ids_ref, weights_ref, info_ref, combine_ref):
    count = ids_ref.shape[0]
    ids, weights = ids_ref[...], weights_ref[...]
    lane = lax.broadcasted_iota(jnp.int32, (count, LANES), 1)
    picks = [ids[:, k : k + 1] == lane for k in range(TOP)]
    chosen = functools.reduce(jnp.logical_or, picks)
    earlier = lax.broadcasted_iota(jnp.int32, (count, count), 0) > lax.broadcasted_iota(
        jnp.int32, (count, count), 1
    )
    rank = jnp.dot(
        jnp.where(earlier, 1.0, 0.0).astype(jnp.bfloat16),
        jnp.where(chosen, 1.0, 0.0).astype(jnp.bfloat16),
        preferred_element_type=jnp.float32,
    )
    info_ref[...] = jnp.where(chosen, rank, 2.0 * count).astype(jnp.bfloat16)
    column = lax.broadcasted_iota(jnp.int32, combine_ref.shape, 1)
    expert = column // (span * GROUP * cap)
    place = (column % cap).astype(jnp.float32)
    total = jnp.zeros(combine_ref.shape, jnp.float32)
    for k in range(TOP):
        own = jnp.sum(jnp.where(picks[k], rank, 0.0), axis=-1, keepdims=True)
        hit = (ids[:, k : k + 1] == expert) & (own == place)
        total = total + jnp.where(hit, weights[:, k : k + 1], 0.0)
    combine_ref[...] = total


def project_kernel(group, *refs):
    token_refs, gain_ref, weight_refs, outs = (
        refs[:group],
        refs[group],
        refs[group + 1 : group + 5],
        refs[group + 5 :],
    )
    me = lax.axis_index("ep")
    rows = jnp.concatenate([ref[...] for ref in token_refs], axis=0)
    total = None
    for k, near in enumerate(NEAR):
        block = me ^ near
        gain = gain_ref[:, aligned(block * LANES, LANES)]
        scaled = (rows[:, k * LANES : (k + 1) * LANES].astype(jnp.float32) * gain).astype(jnp.bfloat16)
        term = jnp.dot(scaled, weight_refs[k][...], preferred_element_type=jnp.float32)
        total = term if total is None else total + term
    count = token_refs[0].shape[0]
    for m, out in enumerate(outs):
        out[...] = total[m * count : (m + 1) * count].astype(out.dtype)


def readout_kernel(group, outer, *refs):
    part_refs = refs[:group]
    tokens_ref, bound_ref, gain_ref, info_ref, state_ref = refs[group : group + 5]
    forget_ref, fresh_ref = refs[group + 5 : group + 7]
    payloads = refs[group + 7 :]
    count = tokens_ref.shape[0]
    proj = bound_ref.shape[1]
    half = outer // 2

    tokens = tokens_ref[...].astype(jnp.float32)
    scale = lax.rsqrt(jnp.mean(tokens * tokens, axis=-1, keepdims=True) + epsilon)
    matrix = spreader(count)
    for head in range(proj // LANES):

        def pick(which):
            at = slice(which * proj + head * LANES, which * proj + (head + 1) * LANES)
            total = part_refs[0][:, at].astype(jnp.float32)
            for ref in part_refs[1:]:
                total = total + ref[:, at].astype(jnp.float32)
            return total * scale

        cols = slice(head * LANES, (head + 1) * LANES)
        bound = bound_ref[:, cols]
        forget = bound + (1.0 - bound) * jax.nn.sigmoid(pick(0))
        fresh = pick(1)
        query = pick(2)
        forget_ref[:, cols] = forget
        fresh_ref[:, cols] = fresh
        kept = spread(query * forget, matrix)
        rows = [
            jnp.sum(kept[:, s * LANES : (s + 1) * LANES] * state_ref[s, head], axis=0, keepdims=True)
            for s in range(count)
        ]
        added = jnp.sum(query * (1.0 - forget), axis=-1, keepdims=True) * fresh
        readout = jnp.concatenate(rows, axis=0) + added
        normed = (
            readout
            * lax.rsqrt(jnp.mean(readout * readout, axis=-1, keepdims=True) + epsilon)
            * gain_ref[:, cols]
        ).astype(jnp.bfloat16)
        for out in payloads:
            out[:, cols] = normed

    core = lax.axis_index("tp")
    place = lax.axis_index("ep") % GROUP
    for m, out in enumerate(payloads):
        for a in range(half):
            block = (core * half + a) * GROUP + (place ^ m)
            out[:, proj + a * LANES : proj + (a + 1) * LANES] = tokens_ref[:, aligned(block * LANES, LANES)]
        out[:, proj + half * LANES :] = info_ref[...]


def update_kernel(forget_ref, fresh_ref, state_ref, new_ref, slot_ref, sems):
    count = forget_ref.shape[0]
    heads = state_ref.shape[1]
    matrix = spreader(count)
    copies = []
    for head in range(heads):
        cols = slice(head * LANES, (head + 1) * LANES)
        kept = spread(forget_ref[:, cols], matrix)
        fresh = fresh_ref[:, cols]
        for s in range(count):
            keep = kept[:, s * LANES : (s + 1) * LANES]
            slot_ref[head, s] = keep * state_ref[s, head] + (1.0 - keep) * fresh[s : s + 1, :]
        copy = pltpu.make_async_copy(slot_ref.at[head], new_ref.at[:, head], sems.at[head])
        copy.start()
        copies.append(copy)
    for copy in copies:
        copy.wait()


def mix_kernel(outer, *refs):
    payloads = refs[:GROUP]
    weights = refs[GROUP : GROUP + outer]
    own_ref, other_ref, resid_ref, info_ref, heads_ref, part_ref = refs[GROUP + outer :]
    me = lax.axis_index("ep")
    core = lax.axis_index("tp")
    place = me % GROUP
    line = me // GROUP
    half = outer // 2
    count = payloads[0].shape[0]
    proj = weights[0].shape[0]
    for m, ref in enumerate(payloads):
        at = aligned((place ^ m) * count, count)
        heads_ref[at, :] = ref[:, :proj]
        resid_ref[at, :] = ref[:, proj : proj + half * LANES]
        info_ref[at, :] = ref[:, proj + half * LANES :]
    heads = heads_ref[...]
    for m, ref in enumerate(weights):
        product = jnp.dot(heads, ref[...], preferred_element_type=jnp.float32)
        part_ref[:, aligned((line ^ m) * LANES, LANES)] = product.astype(jnp.bfloat16)
    size = half * LANES
    own_ref[...] = part_ref[:, aligned(core * size, size)]
    other_ref[...] = part_ref[:, aligned((1 - core) * size, size)]


def dispatch_kernel(span, own_ref, got_ref, resid_ref, info_ref, out_ref, *rest):
    backs, after_ref = rest[:-1], rest[-1]
    mixer = own_ref[...].astype(jnp.float32) + got_ref[...].astype(jnp.float32)
    after_ref[...] = (resid_ref[...].astype(jnp.float32) + mixer).astype(jnp.bfloat16)
    place = lax.axis_index("ep") % GROUP
    count = after_ref.shape[0] // GROUP
    for m, ref in enumerate(backs):
        ref[...] = after_ref[aligned((place ^ m) * count, count), :]
    after = after_ref[...]
    slots = info_ref[...].astype(jnp.float32).T
    rows = out_ref.shape[1]
    cap = rows // GROUP
    row = lax.broadcasted_iota(jnp.int32, (rows, after.shape[0]), 0)
    col = lax.broadcasted_iota(jnp.int32, (rows, after.shape[0]), 1)
    same = (row // cap) == (col // count)
    slot = (row % cap).astype(jnp.float32)
    for e in range(EXPERTS):
        chosen = same & (slots[e : e + 1, :] == slot)
        select = jnp.where(chosen, 1.0, 0.0).astype(jnp.bfloat16)
        picked = jnp.dot(select, after, preferred_element_type=jnp.float32).astype(jnp.bfloat16)
        for sp in range(span):
            out_ref[e * span + sp] = picked


def gather_rows(outer, ref, rows_ref):
    half = outer // 2
    block = ref.shape[1]
    for z in range(outer):
        for q in range(GROUP):
            for a in range(half):
                at = (a * GROUP + q) * LANES
                rows_ref[z * block : (z + 1) * block, at : at + LANES] = ref[
                    z * GROUP + q, :, a * LANES : (a + 1) * LANES
                ].astype(jnp.float32)
    return rows_ref[...]


def half_products(outer, side, ref, gain_ref, gate_ref, up_ref, rows_ref):
    width = rows_ref.shape[1]
    at = aligned(side * width, width)
    values = gather_rows(outer, ref, rows_ref)
    square = jnp.sum(values * values, axis=-1, keepdims=True)
    scaled = (values * gain_ref[:, at]).astype(jnp.bfloat16)
    gate = jnp.dot(scaled, gate_ref[0, at, :], preferred_element_type=jnp.float32)
    up = jnp.dot(scaled, up_ref[0, at, :], preferred_element_type=jnp.float32)
    return square, gate, up


def first_kernel(outer, mine_ref, gain_ref, gate_ref, up_ref, square_ref, gate_out, up_out, rows_ref):
    side = lax.axis_index("tp")
    square, gate, up = half_products(outer, side, mine_ref, gain_ref, gate_ref, up_ref, rows_ref)
    square_ref[...] = jnp.broadcast_to(square, square_ref.shape)
    gate_out[...] = gate
    up_out[...] = up


def pack_half(side, hidden, down_ref, out_ref, block, cap):
    part = out_ref.shape[1]
    width = part * GROUP
    total = jnp.dot(
        hidden, down_ref[0, :, aligned(side * width, width)], preferred_element_type=jnp.float32
    ).astype(jnp.bfloat16)
    shape = (out_ref.shape[0], total.shape[0])
    row = lax.broadcasted_iota(jnp.int32, shape, 0)
    source = (row // block) * cap + row % cap
    piece = (row % block) // cap
    here = source == lax.broadcasted_iota(jnp.int32, shape, 1)
    packed = None
    for k in range(GROUP):
        select = jnp.where(here & (piece == k), 1.0, 0.0).astype(jnp.bfloat16)
        term = jnp.dot(
            select, total[:, k * part : (k + 1) * part], preferred_element_type=jnp.float32
        )
        packed = term if packed is None else packed + term
    out_ref[...] = packed.astype(jnp.bfloat16)


def second_kernel(outer, cap, theirs_ref, gain_ref, gate_ref, up_ref, down_ref, square_ref, gate_part, up_part, hidden_ref, other_ref, rows_ref):
    side = 1 - lax.axis_index("tp")
    width = 2 * rows_ref.shape[1]
    square, gate, up = half_products(outer, side, theirs_ref, gain_ref, gate_ref, up_ref, rows_ref)
    scale = lax.rsqrt((square_ref[:, :1] + square) / width + epsilon)
    gate = (gate_part[...] + gate) * scale
    up = (up_part[...] + up) * scale
    hidden = (jax.nn.silu(gate) * up).astype(jnp.bfloat16)
    hidden_ref[...] = hidden
    pack_half(side, hidden, down_ref, other_ref, GROUP * cap, cap)


def third_kernel(cap, hidden_ref, down_ref, own_ref):
    pack_half(lax.axis_index("tp"), hidden_ref[...], down_ref, own_ref, GROUP * cap, cap)


def combine_kernel(outer, cap, got_ref, weight_ref, *refs):
    afters, out_ref, base_ref = refs[:GROUP], refs[GROUP], refs[GROUP + 1]
    place = lax.axis_index("ep") % GROUP
    half = outer // 2
    for m, ref in enumerate(afters):
        for a in range(half):
            at = (a * GROUP + (place ^ m)) * LANES
            base_ref[:, aligned(at, LANES)] = ref[:, a * LANES : (a + 1) * LANES].astype(jnp.float32)
    weight = weight_ref[...]
    values = got_ref[...]
    _, part = values.shape
    block = GROUP * cap
    count = weight.shape[0]
    piece = (lax.broadcasted_iota(jnp.int32, weight.shape, 1) % block) // cap
    parts = thirds(weight)
    for k in range(GROUP):
        split = [jnp.where(piece == k, w.astype(jnp.float32), 0.0) for w in parts]
        stacked = jnp.concatenate(split, axis=0).astype(jnp.bfloat16)
        mix = jnp.dot(stacked, values, preferred_element_type=jnp.float32)
        mix = mix[:count] + mix[count : 2 * count] + mix[2 * count :]
        at = slice(k * part, (k + 1) * part)
        out_ref[:, at] = (base_ref[:, at] + mix).astype(jnp.bfloat16)


def fast_shards(
    tokens,
    mix_gain,
    query_weight,
    forget_weight,
    input_weight,
    lower_bound,
    head_gain,
    out_weight,
    state,
    ffn_gain,
    route_ids,
    route_weights,
    expert_gate,
    expert_up,
    expert_down,
):
    bf16, f32 = jnp.bfloat16, jnp.float32
    ep = lax.axis_size("ep")
    count, width = tokens.shape
    heads, size = state.shape[1], state.shape[2]
    proj = query_weight.shape[1]
    outer = ep // GROUP
    half = outer // 2
    span = ep // EXPERTS
    coset = [h * 8 + b for h in range(ep // 8) for b in (0, 7)]

    def move(value, mask):
        if not mask:
            return value
        return lax.ppermute(value, "ep", xor_pairs(ep, mask))

    def swap(value):
        return lax.ppermute(value, "tp", [(0, 1), (1, 0)])

    def shaped(*shape, dtype=bf16):
        return jax.ShapeDtypeStruct(shape, dtype)

    packed, *sent = call(
        functools.partial(prep_kernel, coset),
        [pltpu.with_memory_space_constraint(a, pltpu.HBM) for a in (tokens, forget_weight, input_weight, query_weight)],
        [shaped(LANES, 3 * proj)] + [shaped(count, len(NEAR) * LANES)] * len(coset),
        scratch=[pltpu.SemaphoreType.DMA((3 + len(coset) * len(NEAR),))],
        hbm=True,
    )
    weights = [move(packed, near) for near in NEAR]
    token_blocks = [move(value, mask) for value, mask in zip(sent, coset)]
    out_weights = [move(out_weight, GROUP * m) for m in range(outer)]

    cap = 3 * count // 8
    rows_out = GROUP * cap
    info, combine = call(
        functools.partial(route_kernel, cap, span),
        (route_ids, route_weights),
        [shaped(count, LANES), shaped(count, ep * rows_out, dtype=f32)],
    )

    parts = call(
        functools.partial(project_kernel, len(coset)),
        (*token_blocks, mix_gain.reshape(1, width), *weights),
        [shaped(count, 3 * proj)] * len(coset),
    )
    parts = [move(value, mask) for value, mask in zip(parts, coset)]

    pay = proj + half * LANES + LANES
    args = (
        *parts,
        tokens,
        lower_bound.reshape(1, proj),
        head_gain.reshape(1, proj),
        info,
        state,
    )
    forget, fresh, *payloads = call(
        functools.partial(readout_kernel, len(coset), outer),
        args,
        [shaped(count, proj, dtype=f32)] * 2 + [shaped(count, pay)] * GROUP,
    )
    payloads = [move(value, m) for m, value in enumerate(payloads)]
    vmem = pl.BlockSpec(memory_space=pltpu.VMEM)
    new_state = pl.pallas_call(
        update_kernel,
        out_shape=shaped(*state.shape, dtype=f32),
        in_specs=[vmem] * 3,
        out_specs=pl.BlockSpec(memory_space=pltpu.HBM),
        scratch_shapes=[
            pltpu.VMEM((heads, count, size, size), f32),
            pltpu.SemaphoreType.DMA((heads,)),
        ],
        compiler_params=pltpu.CompilerParams(vmem_limit_bytes=12 << 20),
        cost_estimate=pl.CostEstimate(flops=1_000_000_000, bytes_accessed=100_000, transcendentals=0),
    )(forget, fresh, state)

    tall = GROUP * count
    own, other, resid, infos = call(
        functools.partial(mix_kernel, outer),
        (*payloads, *out_weights),
        [shaped(tall, half * LANES)] * 3 + [shaped(tall, LANES)],
        scratch=[pltpu.VMEM((tall, proj), bf16), pltpu.VMEM((tall, outer * LANES), bf16)],
    )
    got = swap(other)
    outgoing, *afters = call(
        functools.partial(dispatch_kernel, span),
        (own, got, resid, infos),
        [shaped(ep, rows_out, half * LANES)] + [shaped(count, half * LANES)] * GROUP,
        scratch=[pltpu.VMEM((tall, half * LANES), bf16)],
    )
    slot_rows = lax.all_to_all(outgoing, "ep", split_axis=0, concat_axis=0, tiled=True)
    afters = [move(value, m) for m, value in enumerate(afters)]
    other_rows = swap(slot_rows)

    total_rows = ep * cap
    tall = ep * rows_out
    part = width // 2 // GROUP
    wide = expert_gate.shape[2]
    gain = ffn_gain.reshape(1, width)
    rows_scratch = [pltpu.VMEM((total_rows, width // 2), f32)]
    square, gate_part, up_part = call(
        functools.partial(first_kernel, outer),
        (slot_rows, gain, expert_gate, expert_up),
        [shaped(total_rows, LANES, dtype=f32)] + [shaped(total_rows, wide, dtype=f32)] * 2,
        scratch=rows_scratch,
        mib=14,
        flops=100_000_000,
    )
    hidden, theirs = call(
        functools.partial(second_kernel, outer, cap),
        (other_rows, gain, expert_gate, expert_up, expert_down, square, gate_part, up_part),
        [shaped(total_rows, wide), shaped(tall, part)],
        scratch=rows_scratch,
        mib=20,
    )
    theirs = swap(theirs)
    mine = call(
        functools.partial(third_kernel, cap),
        (hidden, expert_down),
        [shaped(tall, part)],
        mib=10,
    )[0]
    reduced = (mine.astype(f32) + theirs.astype(f32)).astype(bf16)
    returned = lax.all_to_all(
        reduced.reshape(ep, rows_out, part), "ep", split_axis=0, concat_axis=0, tiled=True
    )
    mixed_out = call(
        functools.partial(combine_kernel, outer, cap),
        (returned.reshape(tall, part), combine, *afters),
        shaped(count, width // 2),
        scratch=[pltpu.VMEM((count, width // 2), f32)],
    )
    return (mixed_out, new_state)


def rms_scale(values_in, gain_vec):
    return (
        values_in
        * lax.rsqrt(jnp.mean(values_in * values_in, axis=-1, keepdims=True) + epsilon)
        * gain_vec
    )


def slot_ranks(block_ids, expert_count):
    onehot = (block_ids[..., None] == jnp.arange(expert_count, dtype=jnp.int32)).astype(jnp.int32)
    before = jnp.cumsum(onehot, axis=1) - onehot
    return jnp.sum(before * onehot, axis=-1)


def general_shards(
    tokens,
    mix_gain,
    query_weight,
    forget_weight,
    input_weight,
    lower_bound,
    head_gain,
    out_weight,
    state,
    ffn_gain,
    route_ids,
    route_weights,
    expert_gate,
    expert_up,
    expert_down,
):
    seq_dev = tokens.shape[0]
    model_width = tokens.shape[1]
    ep_count = lax.axis_size("ep")
    residual = tokens.astype(jnp.float32)
    normed = rms_scale(residual, mix_gain).astype(jnp.bfloat16)
    head_count = state.shape[1]
    head_size = state.shape[2]
    proj_width = query_weight.shape[1]
    pieces = (
        lax.all_gather(query_weight, "ep", axis=0, tiled=True),
        lax.all_gather(forget_weight, "ep", axis=0, tiled=True),
        lax.all_gather(input_weight, "ep", axis=0, tiled=True),
    )
    queries, forget_pre, fresh_values = tuple(
        (jnp.dot(normed, weight_rows, preferred_element_type=jnp.float32) for weight_rows in pieces)
    )
    forget = (lower_bound + (1.0 - lower_bound) * jax.nn.sigmoid(forget_pre)).reshape(
        seq_dev, head_count, head_size
    )
    queries = queries.reshape(seq_dev, head_count, head_size)
    fresh_values = fresh_values.reshape(seq_dev, head_count, head_size)
    new_state = forget[..., None] * state + (1.0 - forget)[..., None] * fresh_values[:, :, None, :]
    readout = jnp.einsum("shk,shkv->shv", queries, new_state, precision=lax.Precision.HIGHEST)
    readout = rms_scale(readout, head_gain.reshape(head_count, head_size))
    heads_out = readout.reshape(seq_dev, proj_width).astype(jnp.bfloat16)
    partial_mix = jnp.dot(
        heads_out,
        lax.all_gather(out_weight, "ep", axis=1, tiled=True),
        preferred_element_type=jnp.float32,
    )
    mixer_sum = lax.psum(partial_mix.astype(jnp.bfloat16), "tp").astype(jnp.float32)
    after_mixer = (residual + mixer_sum).astype(jnp.bfloat16)
    ffn_in = rms_scale(after_mixer.astype(jnp.float32), ffn_gain).astype(jnp.bfloat16)
    capacity = 3 * seq_dev // 8
    expert_span = ep_count // EXPERTS
    half_width = model_width // lax.axis_size("tp")
    own_columns = lax.dynamic_slice_in_dim(
        after_mixer, lax.axis_index("tp") * half_width, half_width, 1
    ).astype(jnp.float32)
    gate_slice = expert_gate[0]
    up_slice = expert_up[0]
    down_slice = expert_down[0]
    slot_iota = jnp.arange(capacity, dtype=jnp.int32)
    own_rank = slot_ranks(route_ids.reshape(1, seq_dev * TOP), EXPERTS).reshape(seq_dev, TOP)
    expert_iota = jnp.arange(EXPERTS, dtype=jnp.int32)
    chosen = (route_ids[:, :, None, None] == expert_iota[None, None, :, None]) & (
        own_rank[:, :, None, None] == slot_iota[None, None, None, :]
    )
    dispatch = jnp.any(chosen, axis=1).astype(jnp.bfloat16)
    combine = jnp.sum(chosen.astype(jnp.float32) * route_weights[:, :, None, None], axis=1)
    outgoing = jnp.einsum(
        "tec,td->ecd", dispatch, ffn_in, preferred_element_type=jnp.float32
    ).astype(jnp.bfloat16)
    outgoing = jnp.broadcast_to(
        outgoing[:, None], (EXPERTS, expert_span, capacity, model_width)
    ).reshape(ep_count, capacity, model_width)
    slot_rows = lax.all_to_all(outgoing, "ep", split_axis=0, concat_axis=0, tiled=True)
    gate_pre = jnp.einsum(
        "...d,df->...f", slot_rows, gate_slice, preferred_element_type=jnp.float32
    )
    up_pre = jnp.einsum("...d,df->...f", slot_rows, up_slice, preferred_element_type=jnp.float32)
    hidden = (jax.nn.silu(gate_pre) * up_pre).astype(jnp.bfloat16)
    partial_out = jnp.einsum(
        "...f,fd->...d", hidden, down_slice, preferred_element_type=jnp.float32
    )
    reduced = lax.psum_scatter(
        partial_out.astype(jnp.bfloat16), "tp", scatter_dimension=2, tiled=True
    ).astype(jnp.float32)
    returned = lax.all_to_all(
        reduced.astype(jnp.bfloat16), "ep", split_axis=0, concat_axis=0, tiled=True
    ).astype(reduced.dtype)
    expert_out = jnp.sum(returned.reshape(EXPERTS, expert_span, capacity, half_width), axis=1)
    expert_mix = jnp.einsum("tec,ecd->td", combine, expert_out, precision=lax.Precision.HIGHEST)
    mixed_out = (own_columns + expert_mix).astype(jnp.bfloat16)
    return (mixed_out, new_state)


def shards(*args):
    tokens, query_weight, state = args[0], args[2], args[8]
    ep, tp = lax.axis_size("ep"), lax.axis_size("tp")
    fits = (
        tp == 2
        and ep % 8 == 0
        and ep % EXPERTS == 0
        and tokens.shape[0] % 16 == 0
        and 3 * tokens.shape[0] // 8 % 2 == 0
        and tokens.shape[1] == ep * LANES
        and query_weight.shape[0] == LANES
        and state.shape[2:] == (LANES, LANES)
        and args[12].shape[2] % (4 * LANES) == 0
    )
    if not fits:
        return general_shards(*args)
    return fast_shards(*args)


def solution(mesh):
    return jax.shard_map(
        shards,
        mesh=mesh,
        in_specs=(
            P("ep", None),
            P(),
            P("ep", "tp"),
            P("ep", "tp"),
            P("ep", "tp"),
            P("tp"),
            P("tp"),
            P("tp", "ep"),
            P("ep", "tp", None, None),
            P(),
            P("ep", None),
            P("ep", None),
            P("ep", None, "tp"),
            P("ep", None, "tp"),
            P("ep", "tp", None),
        ),
        out_specs=(P("ep", "tp"), P("ep", "tp", None, None)),
        check_vma=False,
    )
```

```python
import functools

import jax
import jax.numpy as jnp
from jax import lax
from jax.experimental import pallas as pl
from jax.experimental.pallas import tpu as pltpu
from jax.sharding import PartitionSpec as P


EXPERTS = 8
TOP = 2
LANES = 128


epsilon = 1e-06

NEAR = (0, 1, 2, 4)
GROUP = 4


def xor_pairs(count, mask):
    return [(i, i ^ mask) for i in range(count)]


def aligned(start, size):
    return pl.ds(pl.multiple_of(start, size), size)


def call(kernel, args, outs, scratch=(), flops=3_000_000_000, traffic=100_000, mib=4, hbm=False):
    vmem = pl.BlockSpec(memory_space=pltpu.VMEM)
    return pl.pallas_call(
        kernel,
        out_shape=outs,
        in_specs=[pl.BlockSpec(memory_space=pltpu.HBM) if hbm else vmem] * len(args),
        out_specs=[vmem] * len(outs) if isinstance(outs, list) else vmem,
        scratch_shapes=list(scratch),
        compiler_params=pltpu.CompilerParams(vmem_limit_bytes=mib << 20),
        cost_estimate=pl.CostEstimate(flops=flops, bytes_accessed=traffic, transcendentals=0),
    )(*args)


def thirds(values):
    high = values.astype(jnp.bfloat16)
    rest = values - high.astype(jnp.float32)
    middle = rest.astype(jnp.bfloat16)
    low = (rest - middle.astype(jnp.float32)).astype(jnp.bfloat16)
    return high, middle, low


def spreader(count):
    shape = (3 * count, count * LANES)
    row = lax.broadcasted_iota(jnp.int32, shape, 0) % count
    col = lax.broadcasted_iota(jnp.int32, shape, 1) // LANES
    return jnp.where(row == col, 1.0, 0.0).astype(jnp.bfloat16)


def spread(values, matrix):
    return lax.dot_general(
        jnp.concatenate([part.astype(jnp.float32) for part in thirds(values)], axis=0).astype(jnp.bfloat16),
        matrix,
        (((0,), (0,)), ((), ())),
        preferred_element_type=jnp.float32,
    )


def prep_kernel(coset, tokens_ref, *refs):
    weight_refs, packed_ref, outs, sems = refs[:3], refs[3], refs[4:-1], refs[-1]
    me = lax.axis_index("ep")
    copies = []

    def start(source, target):
        copy = pltpu.make_async_copy(source, target, sems.at[len(copies)])
        copy.start()
        copies.append(copy)

    for k, ref in enumerate(weight_refs):
        size = ref.shape[1]
        start(ref, packed_ref.at[:, k * size : (k + 1) * size])
    for mask, out in zip(coset, outs):
        for k, near in enumerate(NEAR):
            block = me ^ (mask ^ near)
            start(
                tokens_ref.at[:, aligned(block * LANES, LANES)],
                out.at[:, k * LANES : (k + 1) * LANES],
            )
    for copy in copies:
        copy.wait()


def route_kernel(cap, span, ids_ref, weights_ref, info_ref, combine_ref, matrix_ref):
    matrix_ref[...] = spreader(ids_ref.shape[0])
    count = ids_ref.shape[0]
    ids, weights = ids_ref[...], weights_ref[...]
    lane = lax.broadcasted_iota(jnp.int32, (count, LANES), 1)
    picks = [ids[:, k : k + 1] == lane for k in range(TOP)]
    chosen = functools.reduce(jnp.logical_or, picks)
    earlier = lax.broadcasted_iota(jnp.int32, (count, count), 0) > lax.broadcasted_iota(
        jnp.int32, (count, count), 1
    )
    rank = jnp.dot(
        jnp.where(earlier, 1.0, 0.0).astype(jnp.bfloat16),
        jnp.where(chosen, 1.0, 0.0).astype(jnp.bfloat16),
        preferred_element_type=jnp.float32,
    )
    info_ref[...] = jnp.where(chosen, rank, 2.0 * count).astype(jnp.bfloat16)
    column = lax.broadcasted_iota(jnp.int32, combine_ref.shape, 1)
    expert = column // (span * GROUP * cap)
    place = (column % cap).astype(jnp.float32)
    total = jnp.zeros(combine_ref.shape, jnp.float32)
    for k in range(TOP):
        own = jnp.sum(jnp.where(picks[k], rank, 0.0), axis=-1, keepdims=True)
        hit = (ids[:, k : k + 1] == expert) & (own == place)
        total = total + jnp.where(hit, weights[:, k : k + 1], 0.0)
    combine_ref[...] = total


def project_kernel(group, *refs):
    token_refs, gain_ref, weight_refs, outs = (
        refs[:group],
        refs[group],
        refs[group + 1 : group + 5],
        refs[group + 5 :],
    )
    me = lax.axis_index("ep")
    rows = jnp.concatenate([ref[...] for ref in token_refs], axis=0)
    total = None
    for k, near in enumerate(NEAR):
        block = me ^ near
        gain = gain_ref[:, aligned(block * LANES, LANES)]
        scaled = (rows[:, k * LANES : (k + 1) * LANES].astype(jnp.float32) * gain).astype(jnp.bfloat16)
        term = jnp.dot(scaled, weight_refs[k][...], preferred_element_type=jnp.float32)
        total = term if total is None else total + term
    count = token_refs[0].shape[0]
    for m, out in enumerate(outs):
        out[...] = total[m * count : (m + 1) * count].astype(out.dtype)


def readout_kernel(group, outer, *refs):
    part_refs = refs[:group]
    tokens_ref, bound_ref, gain_ref, info_ref, matrix_ref, state_ref = refs[group : group + 6]
    forget_ref, fresh_ref = refs[group + 6 : group + 8]
    payloads = refs[group + 8 :]
    count = tokens_ref.shape[0]
    proj = bound_ref.shape[1]
    half = outer // 2

    tokens = tokens_ref[...].astype(jnp.float32)
    scale = lax.rsqrt(jnp.mean(tokens * tokens, axis=-1, keepdims=True) + epsilon)
    matrix = matrix_ref[...]
    for head in range(proj // LANES):

        def pick(which):
            at = slice(which * proj + head * LANES, which * proj + (head + 1) * LANES)
            total = part_refs[0][:, at].astype(jnp.float32)
            for ref in part_refs[1:]:
                total = total + ref[:, at].astype(jnp.float32)
            return total * scale

        cols = slice(head * LANES, (head + 1) * LANES)
        bound = bound_ref[:, cols]
        forget = bound + (1.0 - bound) * jax.nn.sigmoid(pick(0))
        fresh = pick(1)
        query = pick(2)
        forget_ref[:, cols] = forget
        fresh_ref[:, cols] = fresh
        kept = spread(query * forget, matrix)
        rows = [
            jnp.sum(kept[:, s * LANES : (s + 1) * LANES] * state_ref[s, head], axis=0, keepdims=True)
            for s in range(count)
        ]
        added = jnp.sum(query * (1.0 - forget), axis=-1, keepdims=True) * fresh
        readout = jnp.concatenate(rows, axis=0) + added
        normed = (
            readout
            * lax.rsqrt(jnp.mean(readout * readout, axis=-1, keepdims=True) + epsilon)
            * gain_ref[:, cols]
        ).astype(jnp.bfloat16)
        for out in payloads:
            out[:, cols] = normed

    core = lax.axis_index("tp")
    place = lax.axis_index("ep") % GROUP
    for m, out in enumerate(payloads):
        for a in range(half):
            block = (core * half + a) * GROUP + (place ^ m)
            out[:, proj + a * LANES : proj + (a + 1) * LANES] = tokens_ref[:, aligned(block * LANES, LANES)]
        out[:, proj + half * LANES :] = info_ref[...]


def update_kernel(forget_ref, fresh_ref, matrix_ref, state_ref, new_ref, slot_ref, sems):
    count = forget_ref.shape[0]
    heads = state_ref.shape[1]
    matrix = matrix_ref[...]
    copies = []
    for head in range(heads):
        cols = slice(head * LANES, (head + 1) * LANES)
        kept = spread(forget_ref[:, cols], matrix)
        fresh = fresh_ref[:, cols]
        for s in range(count):
            keep = kept[:, s * LANES : (s + 1) * LANES]
            slot_ref[head, s] = keep * state_ref[s, head] + (1.0 - keep) * fresh[s : s + 1, :]
        copy = pltpu.make_async_copy(slot_ref.at[head], new_ref.at[:, head], sems.at[head])
        copy.start()
        copies.append(copy)
    for copy in copies:
        copy.wait()


def mix_kernel(outer, *refs):
    payloads = refs[:GROUP]
    weights = refs[GROUP : GROUP + outer]
    own_ref, other_ref, resid_ref, info_ref, heads_ref, part_ref = refs[GROUP + outer :]
    me = lax.axis_index("ep")
    core = lax.axis_index("tp")
    place = me % GROUP
    line = me // GROUP
    half = outer // 2
    count = payloads[0].shape[0]
    proj = weights[0].shape[0]
    for m, ref in enumerate(payloads):
        at = aligned((place ^ m) * count, count)
        heads_ref[at, :] = ref[:, :proj]
        resid_ref[at, :] = ref[:, proj : proj + half * LANES]
        info_ref[at, :] = ref[:, proj + half * LANES :]
    heads = heads_ref[...]
    for m, ref in enumerate(weights):
        product = jnp.dot(heads, ref[...], preferred_element_type=jnp.float32)
        part_ref[:, aligned((line ^ m) * LANES, LANES)] = product.astype(jnp.bfloat16)
    size = half * LANES
    own_ref[...] = part_ref[:, aligned(core * size, size)]
    other_ref[...] = part_ref[:, aligned((1 - core) * size, size)]


def dispatch_kernel(span, own_ref, got_ref, resid_ref, info_ref, out_ref, *rest):
    backs, after_ref = rest[:-1], rest[-1]
    mixer = own_ref[...].astype(jnp.float32) + got_ref[...].astype(jnp.float32)
    after_ref[...] = (resid_ref[...].astype(jnp.float32) + mixer).astype(jnp.bfloat16)
    place = lax.axis_index("ep") % GROUP
    count = after_ref.shape[0] // GROUP
    for m, ref in enumerate(backs):
        ref[...] = after_ref[aligned((place ^ m) * count, count), :]
    after = after_ref[...]
    slots = info_ref[...].astype(jnp.float32).T
    rows = out_ref.shape[1]
    cap = rows // GROUP
    row = lax.broadcasted_iota(jnp.int32, (rows, after.shape[0]), 0)
    col = lax.broadcasted_iota(jnp.int32, (rows, after.shape[0]), 1)
    same = (row // cap) == (col // count)
    slot = (row % cap).astype(jnp.float32)
    for e in range(EXPERTS):
        chosen = same & (slots[e : e + 1, :] == slot)
        select = jnp.where(chosen, 1.0, 0.0).astype(jnp.bfloat16)
        picked = jnp.dot(select, after, preferred_element_type=jnp.float32).astype(jnp.bfloat16)
        for sp in range(span):
            out_ref[e * span + sp] = picked


def gather_rows(outer, ref, rows_ref):
    half = outer // 2
    block = ref.shape[1]
    for z in range(outer):
        for q in range(GROUP):
            for a in range(half):
                at = (a * GROUP + q) * LANES
                rows_ref[z * block : (z + 1) * block, at : at + LANES] = ref[
                    z * GROUP + q, :, a * LANES : (a + 1) * LANES
                ].astype(jnp.float32)
    return rows_ref[...]


def half_products(outer, side, ref, gain_ref, gate_ref, up_ref, rows_ref):
    width = rows_ref.shape[1]
    at = aligned(side * width, width)
    values = gather_rows(outer, ref, rows_ref)
    square = jnp.sum(values * values, axis=-1, keepdims=True)
    scaled = (values * gain_ref[:, at]).astype(jnp.bfloat16)
    gate = jnp.dot(scaled, gate_ref[0, at, :], preferred_element_type=jnp.float32)
    up = jnp.dot(scaled, up_ref[0, at, :], preferred_element_type=jnp.float32)
    return square, gate, up


def first_kernel(outer, mine_ref, gain_ref, gate_ref, up_ref, _, square_ref, gate_out, up_out, rows_ref):
    side = lax.axis_index("tp")
    square, gate, up = half_products(outer, side, mine_ref, gain_ref, gate_ref, up_ref, rows_ref)
    square_ref[...] = jnp.broadcast_to(square, square_ref.shape)
    gate_out[...] = gate
    up_out[...] = up


def pack_half(side, hidden, down_ref, out_ref, total_ref, tall_ref, block, cap):
    part = out_ref.shape[1]
    width = part * GROUP
    owners = out_ref.shape[0] // block
    total = jnp.dot(
        hidden, down_ref[0, :, aligned(side * width, width)], preferred_element_type=jnp.float32
    )
    lanes = part // LANES
    for b in range(width // LANES):
        total_ref[b] = total[:, b * LANES : (b + 1) * LANES]
    for k in range(GROUP):
        for s in range(cap):
            for b in range(lanes):
                tall_ref[b, pl.ds(k * cap + s, owners, stride=block), :] = total_ref[
                    k * lanes + b, pl.ds(s, owners, stride=cap), :
                ]
    for b in range(lanes):
        out_ref[:, b * LANES : (b + 1) * LANES] = tall_ref[b].astype(jnp.bfloat16)


def second_kernel(outer, cap, theirs_ref, gain_ref, gate_ref, up_ref, down_ref, square_ref, gate_part, up_part, hidden_ref, other_ref, rows_ref, total_ref, tall_ref):
    side = 1 - lax.axis_index("tp")
    width = 2 * rows_ref.shape[1]
    square, gate, up = half_products(outer, side, theirs_ref, gain_ref, gate_ref, up_ref, rows_ref)
    scale = lax.rsqrt((square_ref[:, :1] + square) / width + epsilon)
    gate = (gate_part[...] + gate) * scale
    up = (up_part[...] + up) * scale
    hidden = (jax.nn.silu(gate) * up).astype(jnp.bfloat16)
    hidden_ref[...] = hidden
    pack_half(side, hidden, down_ref, other_ref, total_ref, tall_ref, GROUP * cap, cap)


def third_kernel(cap, hidden_ref, down_ref, own_ref, total_ref, tall_ref):
    side = lax.axis_index("tp")
    pack_half(side, hidden_ref[...], down_ref, own_ref, total_ref, tall_ref, GROUP * cap, cap)


def combine_kernel(outer, cap, got_ref, weight_ref, *refs):
    afters, out_ref, base_ref = refs[:GROUP], refs[GROUP], refs[GROUP + 1]
    place = lax.axis_index("ep") % GROUP
    half = outer // 2
    for m, ref in enumerate(afters):
        for a in range(half):
            at = (a * GROUP + (place ^ m)) * LANES
            base_ref[:, aligned(at, LANES)] = ref[:, a * LANES : (a + 1) * LANES].astype(jnp.float32)
    weight = weight_ref[...]
    values = got_ref[...]
    _, part = values.shape
    block = GROUP * cap
    count = weight.shape[0]
    piece = (lax.broadcasted_iota(jnp.int32, weight.shape, 1) % block) // cap
    parts = thirds(weight)
    for k in range(GROUP):
        split = [jnp.where(piece == k, w.astype(jnp.float32), 0.0) for w in parts]
        stacked = jnp.concatenate(split, axis=0).astype(jnp.bfloat16)
        mix = jnp.dot(stacked, values, preferred_element_type=jnp.float32)
        mix = mix[:count] + mix[count : 2 * count] + mix[2 * count :]
        at = slice(k * part, (k + 1) * part)
        out_ref[:, at] = (base_ref[:, at] + mix).astype(jnp.bfloat16)


def fast_shards(
    tokens,
    mix_gain,
    query_weight,
    forget_weight,
    input_weight,
    lower_bound,
    head_gain,
    out_weight,
    state,
    ffn_gain,
    route_ids,
    route_weights,
    expert_gate,
    expert_up,
    expert_down,
):
    bf16, f32 = jnp.bfloat16, jnp.float32
    ep = lax.axis_size("ep")
    count, width = tokens.shape
    heads, size = state.shape[1], state.shape[2]
    proj = query_weight.shape[1]
    outer = ep // GROUP
    half = outer // 2
    span = ep // EXPERTS
    coset = [h * 8 + b for h in range(ep // 8) for b in (0, 7)]

    def move(value, mask):
        if not mask:
            return value
        return lax.ppermute(value, "ep", xor_pairs(ep, mask))

    def swap(value):
        return lax.ppermute(value, "tp", [(0, 1), (1, 0)])

    def shaped(*shape, dtype=bf16):
        return jax.ShapeDtypeStruct(shape, dtype)

    packed, *sent = call(
        functools.partial(prep_kernel, coset),
        [pltpu.with_memory_space_constraint(a, pltpu.HBM) for a in (tokens, forget_weight, input_weight, query_weight)],
        [shaped(LANES, 3 * proj)] + [shaped(count, len(NEAR) * LANES)] * len(coset),
        scratch=[pltpu.SemaphoreType.DMA((3 + len(coset) * len(NEAR),))],
        hbm=True,
    )
    weights = [move(packed, near) for near in NEAR]
    token_blocks = [move(value, mask) for value, mask in zip(sent, coset)]
    out_weights = [move(out_weight, GROUP * m) for m in range(outer)]

    cap = 3 * count // 8
    rows_out = GROUP * cap
    info, combine, matrix = call(
        functools.partial(route_kernel, cap, span),
        (route_ids, route_weights),
        [shaped(count, LANES), shaped(count, ep * rows_out, dtype=f32), shaped(3 * count, count * LANES)],
    )

    parts = call(
        functools.partial(project_kernel, len(coset)),
        (*token_blocks, mix_gain.reshape(1, width), *weights),
        [shaped(count, 3 * proj)] * len(coset),
    )
    parts = [move(value, mask) for value, mask in zip(parts, coset)]

    pay = proj + half * LANES + LANES
    args = (
        *parts,
        tokens,
        lower_bound.reshape(1, proj),
        head_gain.reshape(1, proj),
        info,
        matrix,
        state,
    )
    forget, fresh, *payloads = call(
        functools.partial(readout_kernel, len(coset), outer),
        args,
        [shaped(count, proj, dtype=f32)] * 2 + [shaped(count, pay)] * GROUP,
    )
    payloads = [move(value, m) for m, value in enumerate(payloads)]
    vmem = pl.BlockSpec(memory_space=pltpu.VMEM)
    new_state = pl.pallas_call(
        update_kernel,
        out_shape=shaped(*state.shape, dtype=f32),
        in_specs=[vmem] * 4,
        out_specs=pl.BlockSpec(memory_space=pltpu.HBM),
        scratch_shapes=[
            pltpu.VMEM((heads, count, size, size), f32),
            pltpu.SemaphoreType.DMA((heads,)),
        ],
        compiler_params=pltpu.CompilerParams(vmem_limit_bytes=12 << 20),
        cost_estimate=pl.CostEstimate(flops=1_000_000_000, bytes_accessed=100_000, transcendentals=0),
    )(forget, fresh, matrix, state)

    tall = GROUP * count
    own, other, resid, infos = call(
        functools.partial(mix_kernel, outer),
        (*payloads, *out_weights),
        [shaped(tall, half * LANES)] * 3 + [shaped(tall, LANES)],
        scratch=[pltpu.VMEM((tall, proj), bf16), pltpu.VMEM((tall, outer * LANES), bf16)],
    )
    got = swap(other)
    outgoing, *afters = call(
        functools.partial(dispatch_kernel, span),
        (own, got, resid, infos),
        [shaped(ep, rows_out, half * LANES)] + [shaped(count, half * LANES)] * GROUP,
        scratch=[pltpu.VMEM((tall, half * LANES), bf16)],
    )
    slot_rows = lax.all_to_all(outgoing, "ep", split_axis=0, concat_axis=0, tiled=True)
    afters = [move(value, m) for m, value in enumerate(afters)]
    other_rows = swap(slot_rows)

    total_rows = ep * cap
    tall = ep * rows_out
    part = width // 2 // GROUP
    wide = expert_gate.shape[2]
    gain = ffn_gain.reshape(1, width)
    rows_scratch = [pltpu.VMEM((total_rows, width // 2), f32)]
    pack_scratch = [
        pltpu.VMEM((width // 2 // LANES, total_rows, LANES), f32),
        pltpu.VMEM((part // LANES, tall, LANES), f32),
    ]
    square, gate_part, up_part = call(
        functools.partial(first_kernel, outer),
        (slot_rows, gain, expert_gate, expert_up, expert_down),
        [shaped(total_rows, LANES, dtype=f32)] + [shaped(total_rows, wide, dtype=f32)] * 2,
        scratch=rows_scratch,
        mib=14,
        flops=100_000_000,
    )
    hidden, theirs = call(
        functools.partial(second_kernel, outer, cap),
        (other_rows, gain, expert_gate, expert_up, expert_down, square, gate_part, up_part),
        [shaped(total_rows, wide), shaped(tall, part)],
        scratch=rows_scratch + pack_scratch,
        mib=20,
    )
    theirs = swap(theirs)
    mine = call(
        functools.partial(third_kernel, cap),
        (hidden, expert_down),
        [shaped(tall, part)],
        scratch=pack_scratch,
        mib=10,
    )[0]
    reduced = (mine.astype(f32) + theirs.astype(f32)).astype(bf16)
    returned = lax.all_to_all(
        reduced.reshape(ep, rows_out, part), "ep", split_axis=0, concat_axis=0, tiled=True
    )
    mixed_out = call(
        functools.partial(combine_kernel, outer, cap),
        (returned.reshape(tall, part), combine, *afters),
        shaped(count, width // 2),
        scratch=[pltpu.VMEM((count, width // 2), f32)],
    )
    return (mixed_out, new_state)


def rms_scale(values_in, gain_vec):
    return (
        values_in
        * lax.rsqrt(jnp.mean(values_in * values_in, axis=-1, keepdims=True) + epsilon)
        * gain_vec
    )


def slot_ranks(block_ids, expert_count):
    onehot = (block_ids[..., None] == jnp.arange(expert_count, dtype=jnp.int32)).astype(jnp.int32)
    before = jnp.cumsum(onehot, axis=1) - onehot
    return jnp.sum(before * onehot, axis=-1)


def general_shards(
    tokens,
    mix_gain,
    query_weight,
    forget_weight,
    input_weight,
    lower_bound,
    head_gain,
    out_weight,
    state,
    ffn_gain,
    route_ids,
    route_weights,
    expert_gate,
    expert_up,
    expert_down,
):
    seq_dev = tokens.shape[0]
    model_width = tokens.shape[1]
    ep_count = lax.axis_size("ep")
    residual = tokens.astype(jnp.float32)
    normed = rms_scale(residual, mix_gain).astype(jnp.bfloat16)
    head_count = state.shape[1]
    head_size = state.shape[2]
    proj_width = query_weight.shape[1]
    pieces = (
        lax.all_gather(query_weight, "ep", axis=0, tiled=True),
        lax.all_gather(forget_weight, "ep", axis=0, tiled=True),
        lax.all_gather(input_weight, "ep", axis=0, tiled=True),
    )
    queries, forget_pre, fresh_values = tuple(
        (jnp.dot(normed, weight_rows, preferred_element_type=jnp.float32) for weight_rows in pieces)
    )
    forget = (lower_bound + (1.0 - lower_bound) * jax.nn.sigmoid(forget_pre)).reshape(
        seq_dev, head_count, head_size
    )
    queries = queries.reshape(seq_dev, head_count, head_size)
    fresh_values = fresh_values.reshape(seq_dev, head_count, head_size)
    new_state = forget[..., None] * state + (1.0 - forget)[..., None] * fresh_values[:, :, None, :]
    readout = jnp.einsum("shk,shkv->shv", queries, new_state, precision=lax.Precision.HIGHEST)
    readout = rms_scale(readout, head_gain.reshape(head_count, head_size))
    heads_out = readout.reshape(seq_dev, proj_width).astype(jnp.bfloat16)
    partial_mix = jnp.dot(
        heads_out,
        lax.all_gather(out_weight, "ep", axis=1, tiled=True),
        preferred_element_type=jnp.float32,
    )
    mixer_sum = lax.psum(partial_mix.astype(jnp.bfloat16), "tp").astype(jnp.float32)
    after_mixer = (residual + mixer_sum).astype(jnp.bfloat16)
    ffn_in = rms_scale(after_mixer.astype(jnp.float32), ffn_gain).astype(jnp.bfloat16)
    capacity = 3 * seq_dev // 8
    expert_span = ep_count // EXPERTS
    half_width = model_width // lax.axis_size("tp")
    own_columns = lax.dynamic_slice_in_dim(
        after_mixer, lax.axis_index("tp") * half_width, half_width, 1
    ).astype(jnp.float32)
    gate_slice = expert_gate[0]
    up_slice = expert_up[0]
    down_slice = expert_down[0]
    slot_iota = jnp.arange(capacity, dtype=jnp.int32)
    own_rank = slot_ranks(route_ids.reshape(1, seq_dev * TOP), EXPERTS).reshape(seq_dev, TOP)
    expert_iota = jnp.arange(EXPERTS, dtype=jnp.int32)
    chosen = (route_ids[:, :, None, None] == expert_iota[None, None, :, None]) & (
        own_rank[:, :, None, None] == slot_iota[None, None, None, :]
    )
    dispatch = jnp.any(chosen, axis=1).astype(jnp.bfloat16)
    combine = jnp.sum(chosen.astype(jnp.float32) * route_weights[:, :, None, None], axis=1)
    outgoing = jnp.einsum(
        "tec,td->ecd", dispatch, ffn_in, preferred_element_type=jnp.float32
    ).astype(jnp.bfloat16)
    outgoing = jnp.broadcast_to(
        outgoing[:, None], (EXPERTS, expert_span, capacity, model_width)
    ).reshape(ep_count, capacity, model_width)
    slot_rows = lax.all_to_all(outgoing, "ep", split_axis=0, concat_axis=0, tiled=True)
    gate_pre = jnp.einsum(
        "...d,df->...f", slot_rows, gate_slice, preferred_element_type=jnp.float32
    )
    up_pre = jnp.einsum("...d,df->...f", slot_rows, up_slice, preferred_element_type=jnp.float32)
    hidden = (jax.nn.silu(gate_pre) * up_pre).astype(jnp.bfloat16)
    partial_out = jnp.einsum(
        "...f,fd->...d", hidden, down_slice, preferred_element_type=jnp.float32
    )
    reduced = lax.psum_scatter(
        partial_out.astype(jnp.bfloat16), "tp", scatter_dimension=2, tiled=True
    ).astype(jnp.float32)
    returned = lax.all_to_all(
        reduced.astype(jnp.bfloat16), "ep", split_axis=0, concat_axis=0, tiled=True
    ).astype(reduced.dtype)
    expert_out = jnp.sum(returned.reshape(EXPERTS, expert_span, capacity, half_width), axis=1)
    expert_mix = jnp.einsum("tec,ecd->td", combine, expert_out, precision=lax.Precision.HIGHEST)
    mixed_out = (own_columns + expert_mix).astype(jnp.bfloat16)
    return (mixed_out, new_state)


def shards(*args):
    tokens, query_weight, state = args[0], args[2], args[8]
    ep, tp = lax.axis_size("ep"), lax.axis_size("tp")
    fits = (
        tp == 2
        and ep % 8 == 0
        and ep % EXPERTS == 0
        and tokens.shape[0] % 16 == 0
        and 3 * tokens.shape[0] // 8 % 2 == 0
        and tokens.shape[1] == ep * LANES
        and query_weight.shape[0] == LANES
        and state.shape[2:] == (LANES, LANES)
        and args[12].shape[2] % (4 * LANES) == 0
    )
    if not fits:
        return general_shards(*args)
    return fast_shards(*args)


def solution(mesh):
    return jax.shard_map(
        shards,
        mesh=mesh,
        in_specs=(
            P("ep", None),
            P(),
            P("ep", "tp"),
            P("ep", "tp"),
            P("ep", "tp"),
            P("tp"),
            P("tp"),
            P("tp", "ep"),
            P("ep", "tp", None, None),
            P(),
            P("ep", None),
            P("ep", None),
            P("ep", None, "tp"),
            P("ep", None, "tp"),
            P("ep", "tp", None),
        ),
        out_specs=(P("ep", "tp"), P("ep", "tp", None, None)),
        check_vma=False,
    )
```

```python
import functools

import jax
import jax.numpy as jnp
from jax import lax
from jax.experimental import pallas as pl
from jax.experimental.pallas import tpu as pltpu
from jax.sharding import PartitionSpec as P


EXPERTS = 8
TOP = 2
LANES = 128


epsilon = 1e-06

NEAR = (0, 1, 2, 4)
GROUP = 4


def xor_pairs(count, mask):
    return [(i, i ^ mask) for i in range(count)]


def aligned(start, size):
    return pl.ds(pl.multiple_of(start, size), size)


def call(kernel, args, outs, scratch=(), flops=3_000_000_000, traffic=100_000, mib=4, hbm=False):
    vmem = pl.BlockSpec(memory_space=pltpu.VMEM)
    return pl.pallas_call(
        kernel,
        out_shape=outs,
        in_specs=[pl.BlockSpec(memory_space=pltpu.HBM) if hbm else vmem] * len(args),
        out_specs=[vmem] * len(outs) if isinstance(outs, list) else vmem,
        scratch_shapes=list(scratch),
        compiler_params=pltpu.CompilerParams(vmem_limit_bytes=mib << 20),
        cost_estimate=pl.CostEstimate(flops=flops, bytes_accessed=traffic, transcendentals=0),
    )(*args)


def thirds(values):
    high = values.astype(jnp.bfloat16)
    rest = values - high.astype(jnp.float32)
    middle = rest.astype(jnp.bfloat16)
    low = (rest - middle.astype(jnp.float32)).astype(jnp.bfloat16)
    return high, middle, low


def spreader(count):
    shape = (3 * count, count * LANES)
    row = lax.broadcasted_iota(jnp.int32, shape, 0) % count
    col = lax.broadcasted_iota(jnp.int32, shape, 1) // LANES
    return jnp.where(row == col, 1.0, 0.0).astype(jnp.bfloat16)


def spread(values, matrix):
    return lax.dot_general(
        jnp.concatenate([part.astype(jnp.float32) for part in thirds(values)], axis=0).astype(jnp.bfloat16),
        matrix,
        (((0,), (0,)), ((), ())),
        preferred_element_type=jnp.float32,
    )


def prep_kernel(coset, tokens_ref, *refs):
    weight_refs, packed_ref, outs, sems = refs[:3], refs[3], refs[4:-1], refs[-1]
    me = lax.axis_index("ep")
    copies = []

    def start(source, target):
        copy = pltpu.make_async_copy(source, target, sems.at[len(copies)])
        copy.start()
        copies.append(copy)

    for k, ref in enumerate(weight_refs):
        size = ref.shape[1]
        start(ref, packed_ref.at[:, k * size : (k + 1) * size])
    for mask, out in zip(coset, outs):
        for k, near in enumerate(NEAR):
            block = me ^ (mask ^ near)
            start(
                tokens_ref.at[:, aligned(block * LANES, LANES)],
                out.at[:, k * LANES : (k + 1) * LANES],
            )
    for copy in copies:
        copy.wait()


def route_kernel(cap, span, ids_ref, weights_ref, tokens_ref, info_ref, combine_ref, matrix_ref, scale_ref):
    tokens = tokens_ref[...].astype(jnp.float32)
    scale = lax.rsqrt(jnp.mean(tokens * tokens, axis=-1, keepdims=True) + epsilon)
    scale_ref[...] = jnp.broadcast_to(scale, scale_ref.shape)
    matrix_ref[...] = spreader(ids_ref.shape[0])
    count = ids_ref.shape[0]
    ids, weights = ids_ref[...], weights_ref[...]
    lane = lax.broadcasted_iota(jnp.int32, (count, LANES), 1)
    picks = [ids[:, k : k + 1] == lane for k in range(TOP)]
    chosen = functools.reduce(jnp.logical_or, picks)
    earlier = lax.broadcasted_iota(jnp.int32, (count, count), 0) > lax.broadcasted_iota(
        jnp.int32, (count, count), 1
    )
    rank = jnp.dot(
        jnp.where(earlier, 1.0, 0.0).astype(jnp.bfloat16),
        jnp.where(chosen, 1.0, 0.0).astype(jnp.bfloat16),
        preferred_element_type=jnp.float32,
    )
    info_ref[...] = jnp.where(chosen, rank, 2.0 * count).astype(jnp.bfloat16)
    column = lax.broadcasted_iota(jnp.int32, combine_ref.shape, 1)
    expert = column // (span * GROUP * cap)
    place = (column % cap).astype(jnp.float32)
    total = jnp.zeros(combine_ref.shape, jnp.float32)
    for k in range(TOP):
        own = jnp.sum(jnp.where(picks[k], rank, 0.0), axis=-1, keepdims=True)
        hit = (ids[:, k : k + 1] == expert) & (own == place)
        total = total + jnp.where(hit, weights[:, k : k + 1], 0.0)
    combine_ref[...] = total


def project_kernel(group, *refs):
    token_refs, gain_ref, weight_refs, outs = (
        refs[:group],
        refs[group],
        refs[group + 1 : group + 5],
        refs[group + 5 :],
    )
    me = lax.axis_index("ep")
    rows = jnp.concatenate([ref[...] for ref in token_refs], axis=0)
    total = None
    for k, near in enumerate(NEAR):
        block = me ^ near
        gain = gain_ref[:, aligned(block * LANES, LANES)]
        scaled = (rows[:, k * LANES : (k + 1) * LANES].astype(jnp.float32) * gain).astype(jnp.bfloat16)
        term = jnp.dot(scaled, weight_refs[k][...], preferred_element_type=jnp.float32)
        total = term if total is None else total + term
    count = token_refs[0].shape[0]
    for m, out in enumerate(outs):
        out[...] = total[m * count : (m + 1) * count].astype(out.dtype)


def readout_kernel(group, outer, *refs):
    part_refs = refs[:group]
    tokens_ref, bound_ref, gain_ref, info_ref, matrix_ref, scale_ref, state_ref = refs[group : group + 7]
    forget_ref, fresh_ref = refs[group + 7 : group + 9]
    payloads = refs[group + 9 :]
    count = tokens_ref.shape[0]
    proj = bound_ref.shape[1]
    half = outer // 2

    scale = scale_ref[...]
    matrix = matrix_ref[...]
    for head in range(proj // LANES):

        def pick(which):
            at = slice(which * proj + head * LANES, which * proj + (head + 1) * LANES)
            total = part_refs[0][:, at].astype(jnp.float32)
            for ref in part_refs[1:]:
                total = total + ref[:, at].astype(jnp.float32)
            return total * scale

        cols = slice(head * LANES, (head + 1) * LANES)
        bound = bound_ref[:, cols]
        forget = bound + (1.0 - bound) * jax.nn.sigmoid(pick(0))
        fresh = pick(1)
        query = pick(2)
        forget_ref[:, cols] = forget
        fresh_ref[:, cols] = fresh
        kept = spread(query * forget, matrix)
        rows = [
            jnp.sum(kept[:, s * LANES : (s + 1) * LANES] * state_ref[s, head], axis=0, keepdims=True)
            for s in range(count)
        ]
        added = jnp.sum(query * (1.0 - forget), axis=-1, keepdims=True) * fresh
        readout = jnp.concatenate(rows, axis=0) + added
        normed = (
            readout
            * lax.rsqrt(jnp.mean(readout * readout, axis=-1, keepdims=True) + epsilon)
            * gain_ref[:, cols]
        ).astype(jnp.bfloat16)
        for out in payloads:
            out[:, cols] = normed

    core = lax.axis_index("tp")
    place = lax.axis_index("ep") % GROUP
    for m, out in enumerate(payloads):
        for a in range(half):
            block = (core * half + a) * GROUP + (place ^ m)
            out[:, proj + a * LANES : proj + (a + 1) * LANES] = tokens_ref[:, aligned(block * LANES, LANES)]
        out[:, proj + half * LANES :] = info_ref[...]


def update_kernel(forget_ref, fresh_ref, matrix_ref, state_ref, new_ref, slot_ref, sems):
    count = forget_ref.shape[0]
    heads = state_ref.shape[1]
    matrix = matrix_ref[...]
    copies = []
    for head in range(heads):
        cols = slice(head * LANES, (head + 1) * LANES)
        kept = spread(forget_ref[:, cols], matrix)
        fresh = fresh_ref[:, cols]
        for s in range(count):
            keep = kept[:, s * LANES : (s + 1) * LANES]
            slot_ref[head, s] = keep * state_ref[s, head] + (1.0 - keep) * fresh[s : s + 1, :]
        copy = pltpu.make_async_copy(slot_ref.at[head], new_ref.at[:, head], sems.at[head])
        copy.start()
        copies.append(copy)
    for copy in copies:
        copy.wait()


def mix_kernel(outer, *refs):
    payloads = refs[:GROUP]
    weights = refs[GROUP : GROUP + outer]
    own_ref, other_ref, resid_ref, info_ref, heads_ref, part_ref = refs[GROUP + outer :]
    me = lax.axis_index("ep")
    core = lax.axis_index("tp")
    place = me % GROUP
    line = me // GROUP
    half = outer // 2
    count = payloads[0].shape[0]
    proj = weights[0].shape[0]
    for m, ref in enumerate(payloads):
        at = aligned((place ^ m) * count, count)
        heads_ref[at, :] = ref[:, :proj]
        resid_ref[at, :] = ref[:, proj : proj + half * LANES]
        info_ref[at, :] = ref[:, proj + half * LANES :]
    heads = heads_ref[...]
    for m, ref in enumerate(weights):
        product = jnp.dot(heads, ref[...], preferred_element_type=jnp.float32)
        part_ref[:, aligned((line ^ m) * LANES, LANES)] = product.astype(jnp.bfloat16)
    size = half * LANES
    own_ref[...] = part_ref[:, aligned(core * size, size)]
    other_ref[...] = part_ref[:, aligned((1 - core) * size, size)]


def dispatch_kernel(span, own_ref, got_ref, resid_ref, info_ref, out_ref, *rest):
    backs, after_ref = rest[:-1], rest[-1]
    mixer = own_ref[...].astype(jnp.float32) + got_ref[...].astype(jnp.float32)
    after_ref[...] = (resid_ref[...].astype(jnp.float32) + mixer).astype(jnp.bfloat16)
    place = lax.axis_index("ep") % GROUP
    count = after_ref.shape[0] // GROUP
    for m, ref in enumerate(backs):
        ref[...] = after_ref[aligned((place ^ m) * count, count), :]
    after = after_ref[...]
    slots = info_ref[...].astype(jnp.float32).T
    rows = out_ref.shape[1]
    cap = rows // GROUP
    row = lax.broadcasted_iota(jnp.int32, (rows, after.shape[0]), 0)
    col = lax.broadcasted_iota(jnp.int32, (rows, after.shape[0]), 1)
    same = (row // cap) == (col // count)
    slot = (row % cap).astype(jnp.float32)
    for e in range(EXPERTS):
        chosen = same & (slots[e : e + 1, :] == slot)
        select = jnp.where(chosen, 1.0, 0.0).astype(jnp.bfloat16)
        picked = jnp.dot(select, after, preferred_element_type=jnp.float32).astype(jnp.bfloat16)
        for sp in range(span):
            out_ref[e * span + sp] = picked


def gather_rows(outer, ref, rows_ref):
    half = outer // 2
    block = ref.shape[1]
    for z in range(outer):
        for q in range(GROUP):
            for a in range(half):
                at = (a * GROUP + q) * LANES
                rows_ref[z * block : (z + 1) * block, at : at + LANES] = ref[
                    z * GROUP + q, :, a * LANES : (a + 1) * LANES
                ].astype(jnp.float32)
    return rows_ref[...]


def half_products(outer, side, ref, gain_ref, gate_ref, up_ref, rows_ref):
    width = rows_ref.shape[1]
    at = aligned(side * width, width)
    values = gather_rows(outer, ref, rows_ref)
    square = jnp.sum(values * values, axis=-1, keepdims=True)
    scaled = (values * gain_ref[:, at]).astype(jnp.bfloat16)
    gate = jnp.dot(scaled, gate_ref[0, at, :], preferred_element_type=jnp.float32)
    up = jnp.dot(scaled, up_ref[0, at, :], preferred_element_type=jnp.float32)
    return square, gate, up


def first_kernel(outer, mine_ref, gain_ref, gate_ref, up_ref, _, square_ref, gate_out, up_out, rows_ref):
    side = lax.axis_index("tp")
    square, gate, up = half_products(outer, side, mine_ref, gain_ref, gate_ref, up_ref, rows_ref)
    square_ref[...] = jnp.broadcast_to(square, square_ref.shape)
    gate_out[...] = gate
    up_out[...] = up


def pack_half(side, hidden, down_ref, out_ref, total_ref, tall_ref, block, cap):
    part = out_ref.shape[1]
    width = part * GROUP
    owners = out_ref.shape[0] // block
    total = jnp.dot(
        hidden, down_ref[0, :, aligned(side * width, width)], preferred_element_type=jnp.float32
    )
    lanes = part // LANES
    for b in range(width // LANES):
        total_ref[b] = total[:, b * LANES : (b + 1) * LANES]
    for k in range(GROUP):
        for s in range(cap):
            for b in range(lanes):
                tall_ref[b, pl.ds(k * cap + s, owners, stride=block), :] = total_ref[
                    k * lanes + b, pl.ds(s, owners, stride=cap), :
                ]
    for b in range(lanes):
        out_ref[:, b * LANES : (b + 1) * LANES] = tall_ref[b].astype(jnp.bfloat16)


def second_kernel(outer, cap, theirs_ref, gain_ref, gate_ref, up_ref, down_ref, square_ref, gate_part, up_part, hidden_ref, other_ref, rows_ref, total_ref, tall_ref):
    side = 1 - lax.axis_index("tp")
    width = 2 * rows_ref.shape[1]
    square, gate, up = half_products(outer, side, theirs_ref, gain_ref, gate_ref, up_ref, rows_ref)
    scale = lax.rsqrt((square_ref[:, :1] + square) / width + epsilon)
    gate = (gate_part[...] + gate) * scale
    up = (up_part[...] + up) * scale
    hidden = (jax.nn.silu(gate) * up).astype(jnp.bfloat16)
    hidden_ref[...] = hidden
    pack_half(side, hidden, down_ref, other_ref, total_ref, tall_ref, GROUP * cap, cap)


def third_kernel(cap, hidden_ref, down_ref, own_ref, total_ref, tall_ref):
    side = lax.axis_index("tp")
    pack_half(side, hidden_ref[...], down_ref, own_ref, total_ref, tall_ref, GROUP * cap, cap)


def combine_kernel(outer, cap, got_ref, weight_ref, *refs):
    afters, out_ref, base_ref = refs[:GROUP], refs[GROUP], refs[GROUP + 1]
    place = lax.axis_index("ep") % GROUP
    half = outer // 2
    for m, ref in enumerate(afters):
        for a in range(half):
            at = (a * GROUP + (place ^ m)) * LANES
            base_ref[:, aligned(at, LANES)] = ref[:, a * LANES : (a + 1) * LANES].astype(jnp.float32)
    weight = weight_ref[...]
    values = got_ref[...]
    _, part = values.shape
    block = GROUP * cap
    count = weight.shape[0]
    piece = (lax.broadcasted_iota(jnp.int32, weight.shape, 1) % block) // cap
    parts = thirds(weight)
    for k in range(GROUP):
        split = [jnp.where(piece == k, w.astype(jnp.float32), 0.0) for w in parts]
        stacked = jnp.concatenate(split, axis=0).astype(jnp.bfloat16)
        mix = jnp.dot(stacked, values, preferred_element_type=jnp.float32)
        mix = mix[:count] + mix[count : 2 * count] + mix[2 * count :]
        at = slice(k * part, (k + 1) * part)
        out_ref[:, at] = (base_ref[:, at] + mix).astype(jnp.bfloat16)


def fast_shards(
    tokens,
    mix_gain,
    query_weight,
    forget_weight,
    input_weight,
    lower_bound,
    head_gain,
    out_weight,
    state,
    ffn_gain,
    route_ids,
    route_weights,
    expert_gate,
    expert_up,
    expert_down,
):
    bf16, f32 = jnp.bfloat16, jnp.float32
    ep = lax.axis_size("ep")
    count, width = tokens.shape
    heads, size = state.shape[1], state.shape[2]
    proj = query_weight.shape[1]
    outer = ep // GROUP
    half = outer // 2
    span = ep // EXPERTS
    coset = [h * 8 + b for h in range(ep // 8) for b in (0, 7)]

    def move(value, mask):
        if not mask:
            return value
        return lax.ppermute(value, "ep", xor_pairs(ep, mask))

    def swap(value):
        return lax.ppermute(value, "tp", [(0, 1), (1, 0)])

    def shaped(*shape, dtype=bf16):
        return jax.ShapeDtypeStruct(shape, dtype)

    packed, *sent = call(
        functools.partial(prep_kernel, coset),
        [pltpu.with_memory_space_constraint(a, pltpu.HBM) for a in (tokens, forget_weight, input_weight, query_weight)],
        [shaped(LANES, 3 * proj)] + [shaped(count, len(NEAR) * LANES)] * len(coset),
        scratch=[pltpu.SemaphoreType.DMA((3 + len(coset) * len(NEAR),))],
        hbm=True,
    )
    weights = [move(packed, near) for near in NEAR]
    token_blocks = [move(value, mask) for value, mask in zip(sent, coset)]
    out_weights = [move(out_weight, GROUP * m) for m in range(outer)]

    cap = 3 * count // 8
    rows_out = GROUP * cap
    info, combine, matrix, scale = call(
        functools.partial(route_kernel, cap, span),
        (route_ids, route_weights, tokens),
        [shaped(count, LANES), shaped(count, ep * rows_out, dtype=f32), shaped(3 * count, count * LANES), shaped(count, LANES, dtype=f32)],
    )

    parts = call(
        functools.partial(project_kernel, len(coset)),
        (*token_blocks, mix_gain.reshape(1, width), *weights),
        [shaped(count, 3 * proj)] * len(coset),
    )
    parts = [move(value, mask) for value, mask in zip(parts, coset)]

    pay = proj + half * LANES + LANES
    args = (
        *parts,
        tokens,
        lower_bound.reshape(1, proj),
        head_gain.reshape(1, proj),
        info,
        matrix,
        scale,
        state,
    )
    forget, fresh, *payloads = call(
        functools.partial(readout_kernel, len(coset), outer),
        args,
        [shaped(count, proj, dtype=f32)] * 2 + [shaped(count, pay)] * GROUP,
    )
    payloads = [move(value, m) for m, value in enumerate(payloads)]
    vmem = pl.BlockSpec(memory_space=pltpu.VMEM)
    new_state = pl.pallas_call(
        update_kernel,
        out_shape=shaped(*state.shape, dtype=f32),
        in_specs=[vmem] * 4,
        out_specs=pl.BlockSpec(memory_space=pltpu.HBM),
        scratch_shapes=[
            pltpu.VMEM((heads, count, size, size), f32),
            pltpu.SemaphoreType.DMA((heads,)),
        ],
        compiler_params=pltpu.CompilerParams(vmem_limit_bytes=12 << 20),
        cost_estimate=pl.CostEstimate(flops=1_000_000_000, bytes_accessed=100_000, transcendentals=0),
    )(forget, fresh, matrix, state)

    tall = GROUP * count
    own, other, resid, infos = call(
        functools.partial(mix_kernel, outer),
        (*payloads, *out_weights),
        [shaped(tall, half * LANES)] * 3 + [shaped(tall, LANES)],
        scratch=[pltpu.VMEM((tall, proj), bf16), pltpu.VMEM((tall, outer * LANES), bf16)],
    )
    got = swap(other)
    outgoing, *afters = call(
        functools.partial(dispatch_kernel, span),
        (own, got, resid, infos),
        [shaped(ep, rows_out, half * LANES)] + [shaped(count, half * LANES)] * GROUP,
        scratch=[pltpu.VMEM((tall, half * LANES), bf16)],
    )
    slot_rows = lax.all_to_all(outgoing, "ep", split_axis=0, concat_axis=0, tiled=True)
    afters = [move(value, m) for m, value in enumerate(afters)]
    other_rows = swap(slot_rows)

    total_rows = ep * cap
    tall = ep * rows_out
    part = width // 2 // GROUP
    wide = expert_gate.shape[2]
    gain = ffn_gain.reshape(1, width)
    rows_scratch = [pltpu.VMEM((total_rows, width // 2), f32)]
    pack_scratch = [
        pltpu.VMEM((width // 2 // LANES, total_rows, LANES), f32),
        pltpu.VMEM((part // LANES, tall, LANES), f32),
    ]
    square, gate_part, up_part = call(
        functools.partial(first_kernel, outer),
        (slot_rows, gain, expert_gate, expert_up, expert_down),
        [shaped(total_rows, LANES, dtype=f32)] + [shaped(total_rows, wide, dtype=f32)] * 2,
        scratch=rows_scratch,
        mib=14,
        flops=100_000_000,
    )
    hidden, theirs = call(
        functools.partial(second_kernel, outer, cap),
        (other_rows, gain, expert_gate, expert_up, expert_down, square, gate_part, up_part),
        [shaped(total_rows, wide), shaped(tall, part)],
        scratch=rows_scratch + pack_scratch,
        mib=20,
    )
    theirs = swap(theirs)
    mine = call(
        functools.partial(third_kernel, cap),
        (hidden, expert_down),
        [shaped(tall, part)],
        scratch=pack_scratch,
        mib=10,
    )[0]
    reduced = (mine.astype(f32) + theirs.astype(f32)).astype(bf16)
    returned = lax.all_to_all(
        reduced.reshape(ep, rows_out, part), "ep", split_axis=0, concat_axis=0, tiled=True
    )
    mixed_out = call(
        functools.partial(combine_kernel, outer, cap),
        (returned.reshape(tall, part), combine, *afters),
        shaped(count, width // 2),
        scratch=[pltpu.VMEM((count, width // 2), f32)],
    )
    return (mixed_out, new_state)


def rms_scale(values_in, gain_vec):
    return (
        values_in
        * lax.rsqrt(jnp.mean(values_in * values_in, axis=-1, keepdims=True) + epsilon)
        * gain_vec
    )


def slot_ranks(block_ids, expert_count):
    onehot = (block_ids[..., None] == jnp.arange(expert_count, dtype=jnp.int32)).astype(jnp.int32)
    before = jnp.cumsum(onehot, axis=1) - onehot
    return jnp.sum(before * onehot, axis=-1)


def general_shards(
    tokens,
    mix_gain,
    query_weight,
    forget_weight,
    input_weight,
    lower_bound,
    head_gain,
    out_weight,
    state,
    ffn_gain,
    route_ids,
    route_weights,
    expert_gate,
    expert_up,
    expert_down,
):
    seq_dev = tokens.shape[0]
    model_width = tokens.shape[1]
    ep_count = lax.axis_size("ep")
    residual = tokens.astype(jnp.float32)
    normed = rms_scale(residual, mix_gain).astype(jnp.bfloat16)
    head_count = state.shape[1]
    head_size = state.shape[2]
    proj_width = query_weight.shape[1]
    pieces = (
        lax.all_gather(query_weight, "ep", axis=0, tiled=True),
        lax.all_gather(forget_weight, "ep", axis=0, tiled=True),
        lax.all_gather(input_weight, "ep", axis=0, tiled=True),
    )
    queries, forget_pre, fresh_values = tuple(
        (jnp.dot(normed, weight_rows, preferred_element_type=jnp.float32) for weight_rows in pieces)
    )
    forget = (lower_bound + (1.0 - lower_bound) * jax.nn.sigmoid(forget_pre)).reshape(
        seq_dev, head_count, head_size
    )
    queries = queries.reshape(seq_dev, head_count, head_size)
    fresh_values = fresh_values.reshape(seq_dev, head_count, head_size)
    new_state = forget[..., None] * state + (1.0 - forget)[..., None] * fresh_values[:, :, None, :]
    readout = jnp.einsum("shk,shkv->shv", queries, new_state, precision=lax.Precision.HIGHEST)
    readout = rms_scale(readout, head_gain.reshape(head_count, head_size))
    heads_out = readout.reshape(seq_dev, proj_width).astype(jnp.bfloat16)
    partial_mix = jnp.dot(
        heads_out,
        lax.all_gather(out_weight, "ep", axis=1, tiled=True),
        preferred_element_type=jnp.float32,
    )
    mixer_sum = lax.psum(partial_mix.astype(jnp.bfloat16), "tp").astype(jnp.float32)
    after_mixer = (residual + mixer_sum).astype(jnp.bfloat16)
    ffn_in = rms_scale(after_mixer.astype(jnp.float32), ffn_gain).astype(jnp.bfloat16)
    capacity = 3 * seq_dev // 8
    expert_span = ep_count // EXPERTS
    half_width = model_width // lax.axis_size("tp")
    own_columns = lax.dynamic_slice_in_dim(
        after_mixer, lax.axis_index("tp") * half_width, half_width, 1
    ).astype(jnp.float32)
    gate_slice = expert_gate[0]
    up_slice = expert_up[0]
    down_slice = expert_down[0]
    slot_iota = jnp.arange(capacity, dtype=jnp.int32)
    own_rank = slot_ranks(route_ids.reshape(1, seq_dev * TOP), EXPERTS).reshape(seq_dev, TOP)
    expert_iota = jnp.arange(EXPERTS, dtype=jnp.int32)
    chosen = (route_ids[:, :, None, None] == expert_iota[None, None, :, None]) & (
        own_rank[:, :, None, None] == slot_iota[None, None, None, :]
    )
    dispatch = jnp.any(chosen, axis=1).astype(jnp.bfloat16)
    combine = jnp.sum(chosen.astype(jnp.float32) * route_weights[:, :, None, None], axis=1)
    outgoing = jnp.einsum(
        "tec,td->ecd", dispatch, ffn_in, preferred_element_type=jnp.float32
    ).astype(jnp.bfloat16)
    outgoing = jnp.broadcast_to(
        outgoing[:, None], (EXPERTS, expert_span, capacity, model_width)
    ).reshape(ep_count, capacity, model_width)
    slot_rows = lax.all_to_all(outgoing, "ep", split_axis=0, concat_axis=0, tiled=True)
    gate_pre = jnp.einsum(
        "...d,df->...f", slot_rows, gate_slice, preferred_element_type=jnp.float32
    )
    up_pre = jnp.einsum("...d,df->...f", slot_rows, up_slice, preferred_element_type=jnp.float32)
    hidden = (jax.nn.silu(gate_pre) * up_pre).astype(jnp.bfloat16)
    partial_out = jnp.einsum(
        "...f,fd->...d", hidden, down_slice, preferred_element_type=jnp.float32
    )
    reduced = lax.psum_scatter(
        partial_out.astype(jnp.bfloat16), "tp", scatter_dimension=2, tiled=True
    ).astype(jnp.float32)
    returned = lax.all_to_all(
        reduced.astype(jnp.bfloat16), "ep", split_axis=0, concat_axis=0, tiled=True
    ).astype(reduced.dtype)
    expert_out = jnp.sum(returned.reshape(EXPERTS, expert_span, capacity, half_width), axis=1)
    expert_mix = jnp.einsum("tec,ecd->td", combine, expert_out, precision=lax.Precision.HIGHEST)
    mixed_out = (own_columns + expert_mix).astype(jnp.bfloat16)
    return (mixed_out, new_state)


def shards(*args):
    tokens, query_weight, state = args[0], args[2], args[8]
    ep, tp = lax.axis_size("ep"), lax.axis_size("tp")
    fits = (
        tp == 2
        and ep % 8 == 0
        and ep % EXPERTS == 0
        and tokens.shape[0] % 16 == 0
        and 3 * tokens.shape[0] // 8 % 2 == 0
        and tokens.shape[1] == ep * LANES
        and query_weight.shape[0] == LANES
        and state.shape[2:] == (LANES, LANES)
        and args[12].shape[2] % (4 * LANES) == 0
    )
    if not fits:
        return general_shards(*args)
    return fast_shards(*args)


def solution(mesh):
    return jax.shard_map(
        shards,
        mesh=mesh,
        in_specs=(
            P("ep", None),
            P(),
            P("ep", "tp"),
            P("ep", "tp"),
            P("ep", "tp"),
            P("tp"),
            P("tp"),
            P("tp", "ep"),
            P("ep", "tp", None, None),
            P(),
            P("ep", None),
            P("ep", None),
            P("ep", None, "tp"),
            P("ep", None, "tp"),
            P("ep", "tp", None),
        ),
        out_specs=(P("ep", "tp"), P("ep", "tp", None, None)),
        check_vma=False,
    )
```
